32 devices in a mesh: kv: 8 (over z, y), tp: 4 (over x, core).
Axes of the slice: x: 2, y: 2, z: 4, core: 2. Of those that a mesh axis runs over, the one named last changes fastest.
Arguments:
- residual: bfloat16 [256, 2048], P('kv', 'tp'), may hold values from -12 to 12
- first_gain: bfloat16 [2048], P('tp'), may hold values from 0.099609375 to 1.8984375
- first_gate: bfloat16 [2048, 5632], P('tp', 'kv'), may hold values from -0.125 to 0.125
- first_lift: bfloat16 [2048, 5632], P('tp', 'kv'), may hold values from -0.125 to 0.125
- first_down: bfloat16 [5632, 2048], P('kv', 'tp'), may hold values from -0.078125 to 0.078125
- mixer_gain: bfloat16 [2048], replicated, may hold values from 0.099609375 to 1.8984375
- proj_gate: bfloat16 [2048, 2048], P(None, 'tp'), may hold values from -0.125 to 0.125
- proj_input: bfloat16 [2048, 2048], P(None, 'tp'), may hold values from -0.125 to 0.125
- proj_write: bfloat16 [2048, 1024], P(None, 'tp'), may hold values from -0.125 to 0.125
- proj_read: bfloat16 [2048, 1024], P(None, 'tp'), may hold values from -0.125 to 0.125
- proj_step: bfloat16 [2048, 32], P(None, 'tp'), may hold values from -0.125 to 0.125
- step_bias: float32 [32], P('tp'), may hold values from -5 to -2
- rate_log: float32 [32], P('tp'), may hold values from -0.7 to 2.1
- skip_gain: float32 [32], P('tp'), may hold values from 0.5 to 2
- taps_input: bfloat16 [4, 2048], P(None, 'tp'), may hold values from -3 to 3
- taps_write: bfloat16 [4, 1024], P(None, 'tp'), may hold values from -3 to 3
- taps_read: bfloat16 [4, 1024], P(None, 'tp'), may hold values from -3 to 3
- buffer_input: bfloat16 [256, 3, 2048], P('kv', None, 'tp'), may hold values from -6 to 6
- buffer_write: bfloat16 [256, 3, 1024], P('kv', None, 'tp'), may hold values from -6 to 6
- buffer_read: bfloat16 [256, 3, 1024], P('kv', None, 'tp'), may hold values from -6 to 6
- scan_state: float32 [256, 32, 64, 128], P('kv', 'tp'), may hold values from -1.5 to 1.5
- group_gain: bfloat16 [2048], P('tp'), may hold values from 0.099609375 to 1.8984375
- proj_output: bfloat16 [2048, 2048], P('tp'), may hold values from -0.125 to 0.125
- second_gain: bfloat16 [2048], P('tp'), may hold values from 0.099609375 to 1.8984375
- second_gate: bfloat16 [2048, 5632], P('tp', 'kv'), may hold values from -0.125 to 0.125
- second_lift: bfloat16 [2048, 5632], P('tp', 'kv'), may hold values from -0.125 to 0.125
- second_down: bfloat16 [5632, 2048], P('kv', 'tp'), may hold values from -0.078125 to 0.078125
Outputs:
- residual_out: bfloat16 [256, 2048], P('kv', 'tp')
- state_out: float32 [256, 32, 64, 128], P('kv', 'tp')
The draws below stay inside these ranges and needn't reach their ends.
All inputs are finite; a program needn't handle non-finite values.
Results may differ from the reference program's by a relative error of at most 0.023.
Values may be sent and summed in bfloat16 or wider, within the bound.
A program may use at most 64 MiB of HBM per device.

```python
import jax
import jax.numpy as jnp
from jax import lax

D = 2048
FF = 5632
HEADS = 32
HEAD_DIM = 64
STATE = 128
NGROUPS = 8
CONV = 4
D_SSD = 2048
BATCH = 256
N_TP = 4


def draw_residual(key, part):
    first_key = jax.random.fold_in(key, 0)
    columns = jnp.arange(D, dtype=jnp.float32)
    column_ramp = 0.5 * jnp.power(4.0, columns / (D - 1))
    entries = jax.random.normal(first_key, (BATCH, D), jnp.float32)
    return jnp.clip(entries * column_ramp[None, :], -12.0, 12.0).astype(jnp.bfloat16)


def steps_of(own_key, extent, cuts, least, largest):
    level, own = 1.0, jax.random.fold_in(own_key, 6)
    for position, shards_of in cuts:
        heights = jnp.exp(jax.random.uniform(jax.random.fold_in(own, position), (shards_of,), jnp.float32, least / len(cuts), largest / len(cuts)))
        level = level * jnp.repeat(heights, extent[position] // shards_of).reshape([-1 if axis == position else 1 for axis in range(len(extent))])
    return level


def gaussian(key, dims, width, most, shards=(), held_as=jnp.bfloat16):
    level = steps_of(key, dims, shards, -0.22, 0.18) if shards else 1.0
    values = jax.random.normal(key, dims, jnp.float32) * width * level
    return jnp.minimum(jnp.maximum(values, -most), most).astype(held_as)


def setup_inputs(seed: int = 0) -> dict:
    seeds = jax.random.split(jax.random.key(seed), 28)
    return {
        "residual": draw_residual(jax.random.fold_in(seeds[27], 71), 0),
        "first_gain": jnp.clip(1.0 + 0.18 * jax.random.normal(seeds[1], (D,), jnp.float32), 0.099609375, 1.8984375).astype(jnp.bfloat16),
        "first_gate": gaussian(seeds[2], (D, FF), D ** -0.5, 0.125, ((0, 4), (1, 8))),
        "first_lift": gaussian(seeds[3], (D, FF), D ** -0.5, 0.125, ((0, 4), (1, 8))),
        "first_down": gaussian(seeds[4], (FF, D), FF ** -0.5, 0.078125, ((0, 8), (1, 4))),
        "mixer_gain": jnp.clip(1.0 + 0.18 * jax.random.normal(seeds[5], (D,), jnp.float32), 0.099609375, 1.8984375).astype(jnp.bfloat16),
        "proj_gate": gaussian(seeds[6], (D, D_SSD), D ** -0.5, 0.125, ((1, 4),)),
        "proj_input": gaussian(seeds[7], (D, D_SSD), D ** -0.5, 0.125, ((1, 4),)),
        "proj_write": gaussian(seeds[8], (D, NGROUPS * STATE), D ** -0.5, 0.125, ((1, 4),)),
        "proj_read": gaussian(seeds[9], (D, NGROUPS * STATE), D ** -0.5, 0.125, ((1, 4),)),
        "proj_step": gaussian(seeds[10], (D, HEADS), D ** -0.5, 0.125, ((1, 4),)),
        "step_bias": jnp.clip(-5.0 + 3.0 * jax.random.uniform(seeds[11], (HEADS,), jnp.float32) ** steps_of(seeds[11], (HEADS,), ((0, 4),), -0.2, 0.2), -5.0, -2.0),
        "rate_log": jnp.clip(-0.7 + 2.8 * jax.random.uniform(seeds[12], (HEADS,), jnp.float32) ** steps_of(seeds[12], (HEADS,), ((0, 4),), -0.2, 0.2), -0.7, 2.1),
        "skip_gain": jnp.clip(0.5 + 1.5 * jax.random.uniform(seeds[13], (HEADS,), jnp.float32) ** steps_of(seeds[13], (HEADS,), ((0, 4),), -0.2, 0.2), 0.5, 2.0),
        "taps_input": gaussian(seeds[14], (CONV, D_SSD), CONV ** -0.5, 3.0, ((1, 4),)),
        "taps_write": gaussian(seeds[15], (CONV, NGROUPS * STATE), CONV ** -0.5, 3.0, ((1, 4),)),
        "taps_read": gaussian(seeds[16], (CONV, NGROUPS * STATE), CONV ** -0.5, 3.0, ((1, 4),)),
        "buffer_input": gaussian(seeds[17], (BATCH, CONV - 1, D_SSD), 1.0, 6.0, ((0, 8), (2, 4))),
        "buffer_write": gaussian(seeds[18], (BATCH, CONV - 1, NGROUPS * STATE), 1.0, 6.0, ((0, 8), (2, 4))),
        "buffer_read": gaussian(seeds[19], (BATCH, CONV - 1, NGROUPS * STATE), 1.0, 6.0, ((0, 8), (2, 4))),
        "scan_state": gaussian(seeds[20], (BATCH, HEADS, HEAD_DIM, STATE), 0.1, 1.5, ((0, 8), (1, 4)), jnp.float32),
        "group_gain": jnp.clip(1.0 + 0.18 * jax.random.normal(seeds[21], (D_SSD,), jnp.float32), 0.099609375, 1.8984375).astype(jnp.bfloat16),
        "proj_output": gaussian(seeds[22], (D_SSD, D), D_SSD ** -0.5, 0.125, ((0, 4),)),
        "second_gain": jnp.clip(1.0 + 0.18 * jax.random.normal(seeds[23], (D,), jnp.float32), 0.099609375, 1.8984375).astype(jnp.bfloat16),
        "second_gate": gaussian(seeds[24], (D, FF), D ** -0.5, 0.125, ((0, 4), (1, 8))),
        "second_lift": gaussian(seeds[25], (D, FF), D ** -0.5, 0.125, ((0, 4), (1, 8))),
        "second_down": gaussian(seeds[26], (FF, D), FF ** -0.5, 0.078125, ((0, 8), (1, 4))),
    }


norm_eps = 1e-06

def inverse_rms(values):
    return lax.rsqrt(lax.optimization_barrier(jnp.mean(values * values, axis=-1, keepdims=True)) + norm_eps)

def block_sum(activ, weight, pieces):
    seq_rows = activ.shape[0]
    inner = activ.shape[1] // pieces
    widened = lax.optimization_barrier(activ).astype(jnp.float32).reshape(seq_rows, pieces, inner)
    weight_f = weight.astype(jnp.float32).reshape(pieces, inner, weight.shape[1])
    partial_value = jnp.einsum('btk,tkf->tbf', widened, weight_f)
    rounded = lax.optimization_barrier(partial_value.astype(jnp.bfloat16)).astype(jnp.float32)
    return lax.optimization_barrier(jnp.sum(rounded, axis=0))

def half_step(residual, gain, gate_weight, lift_weight, down_weight):
    widened = residual.astype(jnp.float32)
    normed = (widened * inverse_rms(widened) * gain.astype(jnp.float32)).astype(jnp.bfloat16)
    gate_sum = block_sum(normed, gate_weight, N_TP)
    up_sum = block_sum(normed, lift_weight, N_TP)
    hidden = (jax.nn.silu(gate_sum) * up_sum).astype(jnp.bfloat16)
    branch = jnp.dot(hidden, down_weight, preferred_element_type=jnp.float32)
    return (widened + 0.5 * branch).astype(jnp.bfloat16)

def short_conv(tap_weights, buffer, newest):
    taps_f = tap_weights.astype(jnp.float32)
    summed = lax.optimization_barrier(jnp.sum(buffer.astype(jnp.float32) * taps_f[None, :-1, :], axis=1))
    summed = summed + newest.astype(jnp.float32) * taps_f[-1][None, :]
    return jax.nn.silu(summed)

def state_mixer(residual, mixer_gain, proj_gate, proj_input, proj_write, proj_read, proj_step, step_bias, rate_log, skip_gain, taps_input, taps_write, taps_read, buffer_input, buffer_write, buffer_read, scan_state, group_gain, proj_output):
    seq_rows = residual.shape[0]
    widened = residual.astype(jnp.float32)
    normed = (widened * inverse_rms(widened) * mixer_gain.astype(jnp.float32)).astype(jnp.bfloat16)

    def project(weight):
        return jnp.dot(normed, weight, preferred_element_type=jnp.float32).astype(jnp.bfloat16)
    gate_z = project(proj_gate)
    input_new = project(proj_input)
    write_new = project(proj_write)
    read_new = project(proj_read)
    step_raw = project(proj_step)
    input_conv = short_conv(taps_input, buffer_input, input_new)
    write_conv = short_conv(taps_write, buffer_write, write_new)
    read_conv = short_conv(taps_read, buffer_read, read_new)
    head_count = proj_step.shape[1]
    group_count = proj_write.shape[1] // STATE
    per_group = head_count // group_count
    step = jax.nn.softplus(step_raw.astype(jnp.float32) + step_bias[None, :])
    retain = jnp.exp(-step * jnp.exp(rate_log)[None, :])
    input_heads = input_conv.reshape(seq_rows, group_count, per_group, HEAD_DIM)
    write_groups = write_conv.reshape(seq_rows, group_count, STATE)
    read_groups = read_conv.reshape(seq_rows, group_count, STATE)
    old_state = scan_state.reshape(seq_rows, group_count, per_group, HEAD_DIM, STATE)
    retain_g = retain.reshape(seq_rows, group_count, per_group)
    step_g = step.reshape(seq_rows, group_count, per_group)
    updated = retain_g[..., None, None] * old_state + (step_g[..., None] * input_heads)[..., None] * write_groups[:, :, None, None, :]
    head_out = jnp.einsum('bgrpn,bgn->bgrp', updated, read_groups, precision=lax.Precision.HIGHEST)
    head_out = head_out + skip_gain.reshape(group_count, per_group)[None, :, :, None] * input_heads
    head_short = lax.optimization_barrier(head_out.astype(jnp.bfloat16))
    gated = head_short.astype(jnp.float32).reshape(seq_rows, group_count, per_group * HEAD_DIM)
    gated = gated * jax.nn.silu(gate_z.astype(jnp.float32).reshape(seq_rows, group_count, per_group * HEAD_DIM))
    gated = gated * inverse_rms(gated) * group_gain.astype(jnp.float32).reshape(group_count, per_group * HEAD_DIM)[None]
    gated = gated.reshape(seq_rows, head_count * HEAD_DIM).astype(jnp.bfloat16)
    mixed = block_sum(gated, proj_output, N_TP)
    return ((widened + mixed).astype(jnp.bfloat16), updated.reshape(seq_rows, head_count, HEAD_DIM, STATE))

def reference(residual, first_gain, first_gate, first_lift, first_down, mixer_gain, proj_gate, proj_input, proj_write, proj_read, proj_step, step_bias, rate_log, skip_gain, taps_input, taps_write, taps_read, buffer_input, buffer_write, buffer_read, scan_state, group_gain, proj_output, second_gain, second_gate, second_lift, second_down):
    first = half_step(residual, first_gain, first_gate, first_lift, first_down)
    mixed, state_out = state_mixer(first, mixer_gain, proj_gate, proj_input, proj_write, proj_read, proj_step, step_bias, rate_log, skip_gain, taps_input, taps_write, taps_read, buffer_input, buffer_write, buffer_read, scan_state, group_gain, proj_output)
    residual_out = half_step(mixed, second_gain, second_gate, second_lift, second_down)
    return (residual_out, state_out)
```

```python
import functools

import jax
import jax.numpy as jnp
from jax import lax
from jax.experimental import pallas as pl
from jax.experimental.pallas import tpu as pltpu
from jax.sharding import PartitionSpec as P

HEAD_DIM = 64
STATE = 128
EPS = 1e-06
MESH = pl.DeviceIdType.MESH
F32 = jnp.float32
BF16 = jnp.bfloat16
DMA = pltpu.SemaphoreType.DMA


def silu(v):
    return v / (1.0 + jnp.exp(-v))


def dot(a, b):
    return jnp.dot(a, b, preferred_element_type=F32)


def dot_t(a, b, precision=None):
    return lax.dot_general(a, b, (((1,), (1,)), ((), ())), precision=precision,
                           preferred_element_type=F32)


def far_first(n):
    return sorted(range(1, n), key=lambda d: -min(d, n - d))


def remote(src, dst, send, recv, where):
    return pltpu.make_async_remote_copy(
        src_ref=src, dst_ref=dst, send_sem=send, recv_sem=recv,
        device_id=where, device_id_type=MESH,
    )


class Place:
    def __init__(self, nk, nt):
        self.nk, self.nt, self.nx = nk, nt, nt // 2
        self.kv, self.tp = lax.axis_index("kv"), lax.axis_index("tp")
        self.core = lax.rem(self.tp, 2)
        self.x = lax.div(self.tp, 2)
        self.partner = {"tp": self.tp + 1 - 2 * self.core}

    def kv_to(self, d):
        return lax.rem(self.kv + d, self.nk)

    def kv_from(self, d):
        return lax.rem(self.kv + self.nk - d, self.nk)

    def tp_to(self, d):
        return lax.rem(self.tp + d, self.nt)

    def tp_from(self, d):
        return lax.rem(self.tp + self.nt - d, self.nt)

    def x_to(self, e):
        return lax.rem(self.x + e, self.nx)

    def x_from(self, e):
        return lax.rem(self.x + self.nx - e, self.nx)

    def same_core(self, x):
        return {"tp": 2 * x + self.core}


def enter(p):
    barrier = pltpu.get_barrier_semaphore()
    for d in range(1, p.nk):
        pl.semaphore_signal(barrier, inc=1, device_id={"kv": p.kv_to(d)}, device_id_type=MESH)
    for d in range(1, p.nt):
        pl.semaphore_signal(barrier, inc=1, device_id={"tp": p.tp_to(d)}, device_id_type=MESH)
    pl.semaphore_wait(barrier, p.nk + p.nt - 2)


def half_scratch(nk, nt, rows, width, halfc):
    total, nx = nk * rows, nt // 2
    share = total // nx
    vmem = pltpu.VMEM
    return dict(
        wg=vmem((2, halfc, width), BF16), wu=vmem((2, halfc, width), BF16),
        wd=vmem((2, halfc, width), BF16), wl=DMA((4,)), ws=DMA((2,)), wr=DMA((2,)),
        xall=vmem((total, width), BF16), xg=vmem((2, total, width), BF16),
        ssq=vmem((total, 128), F32),
        sq=vmem((nx, 8, share), F32), sqr=vmem((nt, 8, share), F32),
        part=vmem((nx, 2, share, halfc), BF16), parr=vmem((nx, 2, share, halfc), BF16),
        hid=vmem((2, total, halfc), BF16),
        dpart=vmem((total, width), BF16), dparr=vmem((nk, rows, width), BF16),
        ag_s=DMA((nk,)), ag_r=DMA((nk,)), dd_s=DMA((nk,)), dd_r=DMA((nk,)),
        sq_s=DMA((nt,)), sq_r=DMA((nt,)), rs_s=DMA((nx, 2)), rs_r=DMA((nx, 2)),
        hx_s=DMA((nx,)), hx_r=DMA((nx,)), hd_s=DMA((nx,)), hd_r=DMA((nx,)),
        dn_s=DMA((nk,)), dn_r=DMA((nk,)),
    )


def local_weights(p, s, gate, lift, down):
    copies = [
        pltpu.make_async_copy(gate.at[p.core], s["wg"].at[0], s["wl"].at[0]),
        pltpu.make_async_copy(lift.at[p.core], s["wu"].at[0], s["wl"].at[1]),
        pltpu.make_async_copy(down.at[p.core], s["wd"].at[0], s["wl"].at[2]),
        pltpu.make_async_copy(down.at[1 - p.core], s["wd"].at[1], s["wl"].at[3]),
    ]
    for c in copies:
        c.start()
    return copies


def swap_weights(p, s, gate, lift):
    copies = [
        remote(gate.at[1 - p.core], s["wg"].at[1], s["ws"].at[0], s["wr"].at[0], p.partner),
        remote(lift.at[1 - p.core], s["wu"].at[1], s["ws"].at[1], s["wr"].at[1], p.partner),
    ]
    for c in copies:
        c.start()
    return copies


def half_step(p, s, x_ref, gain, local, swapped, idle):
    nk, nt, nx = p.nk, p.nt, p.nx
    rows, width = x_ref.shape
    total = nk * rows
    share = total // nx
    per = share // rows
    features = width * nt
    sends = []

    def block(k):
        return pl.ds(pl.multiple_of(k * rows, rows), rows)

    def part_rows(x):
        return pl.ds(pl.multiple_of(x * share, share), share)

    gathers = {}
    for d in far_first(nk):
        c = remote(x_ref, s["xall"].at[block(p.kv)], s["ag_s"].at[d], s["ag_r"].at[d],
                   {"kv": p.kv_to(d)})
        c.start()
        gathers[d] = c
    sends += gathers.values()
    idle[0]()
    forwards = []
    for d in [0] + list(reversed(far_first(nk))):
        at = block(p.kv_from(d))
        if d:
            gathers[d].wait_recv()
            value = s["xall"][at, :].astype(F32)
        else:
            value = x_ref[...].astype(F32)
        s["xg"][0, at, :] = (value * gain).astype(BF16)
        c = remote(s["xg"].at[0, at], s["xg"].at[1, at], s["dd_s"].at[d], s["dd_r"].at[d],
                   p.partner)
        c.start()
        forwards.append(c)
        value = value * value
        folded = value[:, :128]
        for i in range(128, width, 128):
            folded = folded + value[:, i:i + 128]
        s["ssq"][at, :] = folded
    sends += forwards
    ones = jnp.ones((8, 128), F32)
    for x in range(nx):
        s["sq"][x] = dot_t(ones, s["ssq"][x * share:(x + 1) * share, :], lax.Precision.HIGHEST)
    squares = []
    for d in far_first(nt):
        to = p.tp_to(d)
        c = remote(s["sq"].at[lax.div(to, 2)], s["sqr"].at[d], s["sq_s"].at[d], s["sq_r"].at[d],
                   {"tp": to})
        c.start()
        squares.append((d, c))
    sends += [c for _, c in squares]
    local[0].wait()
    local[1].wait()
    for c in swapped:
        c.wait_recv()
    for c in forwards:
        c.wait_recv()

    def partial(x, w):
        at = part_rows(x)
        return dot_t(s["xg"][0, at, :], w[0]) + dot_t(s["xg"][1, at, :], w[1])

    parts = {}
    for e in far_first(nx):
        to = p.x_to(e)
        for i, w in enumerate((s["wg"], s["wu"])):
            s["part"][e, i] = partial(to, w).astype(BF16)
            c = remote(s["part"].at[e, i], s["parr"].at[e, i], s["rs_s"].at[e, i],
                       s["rs_r"].at[e, i], p.same_core(to))
            c.start()
            parts[e, i] = c
    sends += parts.values()
    gate = partial(p.x, s["wg"])
    lift = partial(p.x, s["wu"])
    s["part"][0, 0] = gate.astype(BF16)
    s["part"][0, 1] = lift.astype(BF16)
    idle[1]()
    sq = s["sq"][p.x]
    for d, c in squares:
        c.wait_recv()
        sq = sq + s["sqr"][d]
    factor = jnp.transpose(lax.rsqrt(sq / features + EPS))[:, :1]
    gate = s["part"][0, 0].astype(F32)
    lift = s["part"][0, 1].astype(F32)
    for e in reversed(far_first(nx)):
        parts[e, 0].wait_recv()
        gate = gate + s["parr"][e, 0].astype(F32)
    gate = silu(gate * factor) * factor
    for e in reversed(far_first(nx)):
        parts[e, 1].wait_recv()
        lift = lift + s["parr"][e, 1].astype(F32)
    mine = part_rows(p.x)
    s["hid"][0, mine, :] = (gate * lift).astype(BF16)
    spread = {}
    for e in far_first(nx):
        c = remote(s["hid"].at[0, mine], s["hid"].at[0, mine], s["hx_s"].at[e], s["hx_r"].at[e],
                   p.same_core(p.x_to(e)))
        c.start()
        spread[e] = c
    sends += spread.values()
    across = {}

    def forward(e):
        at = part_rows(p.x_from(e))
        c = remote(s["hid"].at[0, at], s["hid"].at[1, at], s["hd_s"].at[e], s["hd_r"].at[e],
                   p.partner)
        c.start()
        across[e] = c

    forward(0)
    local[2].wait()
    local[3].wait()
    order = [0] + list(reversed(far_first(nx)))
    for n, e in enumerate(order):
        source = p.x_from(e)
        at = part_rows(source)
        if e:
            spread[e].wait_recv()
            forward(e)
        mid = dot(s["hid"][0, at, :], s["wd"][0])
        across[e].wait_recv()
        s["dpart"][at, :] = (mid + dot(s["hid"][1, at, :], s["wd"][1])).astype(BF16)
        for j in range(per):
            to = source * per + j

            @pl.when(to != p.kv)
            def _():
                remote(s["dpart"].at[block(to)], s["dparr"].at[p.kv], s["dn_s"].at[to],
                       s["dn_r"].at[p.kv], {"kv": to}).start()

        if n == 0:
            idle[2]()
    sends += across.values()
    idle[3]()
    acc = s["dpart"][block(p.kv), :].astype(F32)
    for d in reversed(far_first(nk)):
        source = p.kv_from(d)
        there = s["dparr"].at[source]
        pltpu.make_async_copy(there, there, s["dn_r"].at[source]).wait()
        acc = acc + s["dparr"][source].astype(F32)

    def finish():
        for d in far_first(nk):
            to = p.kv_to(d)
            there = s["dparr"].at[to]
            pltpu.make_async_copy(there, there, s["dn_s"].at[to]).wait()
        for c in sends + swapped:
            c.wait_send()

    return x_ref[...].astype(F32) + 0.5 * acc, finish


def conv(taps_ref, buf_ref, newest):
    taps = taps_ref[...].astype(F32)
    count = taps.shape[0]
    old = buf_ref[...].astype(F32)
    acc = newest.astype(BF16).astype(F32) * taps[count - 1:count]
    for k in range(count - 1):
        acc = acc + old[k] * taps[k:k + 1]
    return silu(acc)


def split(v):
    high = v.astype(BF16).astype(F32)
    return high, v - high


def layer_kernel(nk, nt, names, *refs):
    r = dict(zip(names, refs))
    p = Place(nk, nt)
    one = {k[2:]: v for k, v in r.items() if k.startswith("1.")}
    two = {k[2:]: v for k, v in r.items() if k.startswith("2.")}
    x_ref, state = r["x"], r["state_out"]
    rows, width = x_ref.shape
    features = nt * width
    chans = r["wx"].shape[-1]
    gs = r["wb"].shape[-1]
    heads = r["ws"].shape[0]
    groups = gs // STATE
    gch = chans // groups
    hg = heads // groups
    wcat = r["wcat"]

    local1 = local_weights(p, one, r["gate1"], r["lift1"], r["down1"])
    mixload = []
    at = 0
    for i, name in enumerate(("wz", "wx", "wb", "wr")):
        w = r[name]
        c = pltpu.make_async_copy(w, wcat.at[:, :, at:at + w.shape[-1]], r["ml"].at[i])
        at += w.shape[-1]
        mixload.append(c)
    mixload.append(pltpu.make_async_copy(r["wo"], r["wov"], r["ml"].at[4]))
    stateload = pltpu.make_async_copy(r["state"], state, r["ml"].at[5])
    enter(p)
    swap1 = swap_weights(p, one, r["gate1"], r["lift1"])

    def row(name):
        return r[name][...].astype(F32).reshape(1, -1)

    later = {}

    def load_rest():
        stateload.start()
        for c in mixload:
            c.start()
        later["local"] = local_weights(p, two, r["gate2"], r["lift2"], r["down2"])
        later["swap"] = swap_weights(p, two, r["gate2"], r["lift2"])

    def narrow():
        stateload.wait()

        def body(i, _):
            for g in range(groups):
                pair = [state[2 * i + j, g * hg:(g + 1) * hg].reshape(gch, STATE)
                        for j in range(2)]
                r["stb"][i, g * gch:(g + 1) * gch, :] = jnp.concatenate(pair, axis=1).astype(BF16)
            return 0

        lax.fori_loop(0, rows // 2, body, 0)

    def nothing():
        pass

    first, finish1 = half_step(p, one, x_ref, row("g1"), local1, swap1,
                               (load_rest, narrow, nothing, nothing))
    held = r["held"]
    held[p.tp] = first.astype(BF16)
    copies = {}
    for d in far_first(nt):
        c = remote(held.at[p.tp], held.at[p.tp], r["f_s"].at[d], r["f_r"].at[d],
                   {"tp": p.tp_to(d)})
        c.start()
        copies[d] = c
    for c in mixload:
        c.wait()
    gm = row("gm")
    gmv = r["gmv"]
    for t in range(nt):
        gmv[t] = gm[:, t * width:(t + 1) * width]
    total = jnp.zeros((rows, 1), F32)
    proj = jnp.zeros((rows, wcat.shape[-1]), F32)
    raw = jnp.zeros((rows, heads), F32)
    for d in [0] + list(reversed(far_first(nt))):
        t = p.tp_from(d)
        if d:
            copies[d].wait_recv()
        v = held[t].astype(F32)
        total = total + jnp.sum(v * v, axis=1, keepdims=True)
        scaled = (v * gmv[t]).astype(BF16)
        proj = proj + dot(scaled, wcat[t])
        raw = raw + dot_t(scaled, r["ws"][:, pl.ds(pl.multiple_of(t * width, width), width)])
    factor = lax.rsqrt(total / features + EPS)
    proj = proj * factor
    raw = (raw * factor).astype(BF16).astype(F32) + r["bias"][...]

    def spread(v):
        a = lax.broadcasted_iota(jnp.int32, (heads, chans), 0)
        c = lax.broadcasted_iota(jnp.int32, (heads, chans), 1)
        ind = jnp.where(c // HEAD_DIM == a, 1.0, 0.0).astype(F32)
        return jnp.dot(v, ind, precision=lax.Precision.HIGHEST, preferred_element_type=F32)

    z = proj[:, :chans].astype(BF16).astype(F32)
    xc = conv(r["tx"], r["bx"], proj[:, chans:2 * chans])
    bc = conv(r["tb"], r["bb"], proj[:, 2 * chans:2 * chans + gs])
    rc = conv(r["tr"], r["br"], proj[:, 2 * chans + gs:])
    step = jnp.maximum(raw, 0.0) + jnp.log1p(jnp.exp(-jnp.abs(raw)))
    retain = jnp.exp(-step * jnp.exp(r["rate"][...]))
    sx = spread(step) * xc
    keep = spread(retain)

    rowid = lax.broadcasted_iota(jnp.int32, (rows, 2 * STATE), 0)
    colid = lax.broadcasted_iota(jnp.int32, (rows, 2 * STATE), 1) // STATE
    pieces = []
    for g in range(groups):
        rg = rc[:, g * STATE:(g + 1) * STATE]
        twice = jnp.concatenate([rg, rg], axis=1)
        acc = jnp.zeros((rows, gch), F32)
        for i in range(rows // 2):
            lhs = jnp.where(rowid - colid == 2 * i, twice, 0.0).astype(BF16)
            acc = acc + dot_t(lhs, r["stb"][i, g * gch:(g + 1) * gch, :])
        br = jnp.sum(bc[:, g * STATE:(g + 1) * STATE] * rg, axis=1, keepdims=True)
        pieces.append(acc * keep[:, g * gch:(g + 1) * gch] + sx[:, g * gch:(g + 1) * gch] * br)
    out = jnp.concatenate(pieces, axis=1) + spread(r["skip"][...]) * xc
    gated = out.astype(BF16).astype(F32) * silu(z)
    pieces = []
    for g in range(groups):
        v = gated[:, g * gch:(g + 1) * gch]
        pieces.append(v * lax.rsqrt(jnp.mean(v * v, axis=1, keepdims=True) + EPS))
    gated = (jnp.concatenate(pieces, axis=1) * row("gg")).astype(BF16)
    pout, arrived = r["pout"], r["arrived"]
    outs = {}
    for d in far_first(nt) + [0]:
        to = p.tp_to(d)
        wo = r["wov"][:, pl.ds(pl.multiple_of(to * width, width), width)]
        pout[d] = dot(gated, wo).astype(BF16)
        if d:
            c = remote(pout.at[d], arrived.at[d], r["m_s"].at[d], r["m_r"].at[d], {"tp": to})
            c.start()
            outs[d] = c

    depth = r["base"].shape[1]
    pad = depth - 5 * rows
    sx_hi, sx_lo = split(sx)
    re_hi, re_lo = split(keep)
    left = jnp.concatenate(
        [sx_hi, sx_lo, sx_hi, re_hi, re_lo, jnp.zeros((pad, chans), F32)], axis=0)
    r["left"][...] = left.T.astype(BF16)
    for g in range(groups):
        b_hi, b_lo = split(bc[:, g * STATE:(g + 1) * STATE])
        zero = jnp.zeros((rows, STATE), F32)
        full = jnp.ones((rows, STATE), F32)
        zpad = jnp.zeros((pad, STATE), F32)
        r["base"][g, :, :STATE] = jnp.concatenate(
            [b_hi, b_hi, b_lo, zero, zero, zpad], axis=0).astype(BF16)
        r["base"][g, :, STATE:] = jnp.concatenate(
            [zero, zero, zero, full, full, zpad], axis=0).astype(BF16)

    acc = held[p.tp].astype(F32) + pout[0].astype(F32)
    for d in reversed(far_first(nt)):
        outs[d].wait_recv()
        acc = acc + arrived[d].astype(F32)
    r["mixed"][...] = acc.astype(BF16)

    rowmod = lax.rem(lax.broadcasted_iota(jnp.int32, (depth, 2 * STATE), 0), rows)

    def update(low, high):
        def body(b, _):
            mask = jnp.where(rowmod == b, 1.0, 0.0).astype(BF16)
            for g in range(groups):
                right = r["base"][g] * mask
                both = dot(r["left"][g * gch:(g + 1) * gch, :], right)
                old = state[b, g * hg:(g + 1) * hg].reshape(gch, STATE)
                new = both[:, STATE:] * old + both[:, :STATE]
                state[b, g * hg:(g + 1) * hg] = new.reshape(hg, HEAD_DIM, STATE)
            return 0

        return lambda: lax.fori_loop(low, high, body, 0)

    last, finish2 = half_step(p, two, r["mixed"], row("g2"), later["local"], later["swap"],
                              (update(0, rows // 2), update(rows // 2, rows), nothing, nothing))
    r["out"][...] = last.astype(BF16)
    finish1()
    finish2()
    for c in list(copies.values()) + list(outs.values()):
        c.wait_send()


def flush_kernel(a, b, oa, ob, sem):
    copies = [pltpu.make_async_copy(a, oa, sem.at[0]), pltpu.make_async_copy(b, ob, sem.at[1])]
    for c in copies:
        c.start()
    for c in copies:
        c.wait()


def per_device(nk, nt, residual, first_gain, first_gate, first_lift, first_down,
               mixer_gain, wz, wx, wb, wr, ws, bias, rate, skip, tx, tb, tr, bx, bb, br,
               state, group_gain, wo, second_gain, second_gate, second_lift, second_down):
    rows, width = residual.shape
    halfc = first_gate.shape[1] // 2
    chans, heads = wx.shape[1], ws.shape[1]
    groups = wb.shape[1] // STATE
    vmem = pltpu.VMEM

    def tall(w):
        return w.T.reshape(2, halfc, width)

    def flip(v):
        return jnp.transpose(v, (1, 0, 2))

    small = dict(x=residual, g1=first_gain, g2=second_gain, gm=mixer_gain, gg=group_gain,
                 ws=ws.T, bias=bias[None, :], rate=rate[None, :], skip=skip[None, :],
                 tx=tx, tb=tb, tr=tr, bx=flip(bx), bb=flip(bb), br=flip(br))
    big = dict(gate1=tall(first_gate), lift1=tall(first_lift),
               down1=first_down.reshape(2, halfc, width),
               gate2=tall(second_gate), lift2=tall(second_lift),
               down2=second_down.reshape(2, halfc, width),
               wz=wz.reshape(nt, width, -1), wx=wx.reshape(nt, width, -1),
               wb=wb.reshape(nt, width, -1), wr=wr.reshape(nt, width, -1), wo=wo, state=state)
    depth = -(-5 * rows // 128) * 128
    scratch = dict(
        wcat=vmem((nt, width, 2 * chans + 2 * groups * STATE), BF16),
        wov=vmem(wo.shape, BF16), ml=DMA((6,)),
        stb=vmem((rows // 2, chans, 2 * STATE), BF16),
        held=vmem((nt, rows, width), BF16), f_s=DMA((nt,)), f_r=DMA((nt,)),
        gmv=vmem((nt, 1, width), F32),
        pout=vmem((nt, rows, width), BF16), arrived=vmem((nt, rows, width), BF16),
        m_s=DMA((nt,)), m_r=DMA((nt,)), mixed=vmem((rows, width), BF16),
        left=vmem((chans, depth), BF16), base=vmem((groups, depth, 2 * STATE), BF16),
    )
    for tag in ("1.", "2."):
        for k, v in half_scratch(nk, nt, rows, width, halfc).items():
            scratch[tag + k] = v
    names = list(small) + list(big) + ["out", "state_out"] + list(scratch)
    inside = pl.BlockSpec(memory_space=pltpu.VMEM)
    outside = pl.BlockSpec(memory_space=pl.ANY)
    out, state_out = pl.pallas_call(
        functools.partial(layer_kernel, nk, nt, names),
        out_shape=(vmem(residual.shape, BF16), vmem(state.shape, F32)),
        in_specs=[inside] * len(small) + [outside] * len(big),
        out_specs=(inside, inside),
        scratch_shapes=list(scratch.values()),
        compiler_params=pltpu.CompilerParams(
            collective_id=1, has_side_effects=True, vmem_limit_bytes=48 * 1024 * 1024),
        name="layer",
    )(*small.values(), *big.values())
    return pl.pallas_call(
        flush_kernel,
        out_shape=(jax.ShapeDtypeStruct(residual.shape, BF16),
                   jax.ShapeDtypeStruct(state.shape, F32)),
        in_specs=[inside] * 2,
        out_specs=(outside, outside),
        scratch_shapes=[DMA((2,))],
        compiler_params=pltpu.CompilerParams(vmem_limit_bytes=1024 * 1024),
        name="flush",
    )(out, state_out)


def solution(mesh):
    placed = (
        P("kv", "tp"),
        P("tp"),
        P("tp", "kv"),
        P("tp", "kv"),
        P("kv", "tp"),
        P(),
        P(None, "tp"),
        P(None, "tp"),
        P(None, "tp"),
        P(None, "tp"),
        P(None, "tp"),
        P("tp"),
        P("tp"),
        P("tp"),
        P(None, "tp"),
        P(None, "tp"),
        P(None, "tp"),
        P("kv", None, "tp"),
        P("kv", None, "tp"),
        P("kv", None, "tp"),
        P("kv", "tp", None, None),
        P("tp"),
        P("tp", None),
        P("tp"),
        P("tp", "kv"),
        P("tp", "kv"),
        P("kv", "tp"),
    )
    return jax.shard_map(
        functools.partial(per_device, mesh.shape["kv"], mesh.shape["tp"]),
        mesh=mesh,
        in_specs=placed,
        out_specs=(P("kv", "tp"), P("kv", "tp", None, None)),
        check_vma=False,
    )
```

```python
import functools

import jax
import jax.numpy as jnp
from jax import lax
from jax.experimental import pallas as pl
from jax.experimental.pallas import tpu as pltpu
from jax.sharding import PartitionSpec as P

HEAD_DIM = 64
STATE = 128
EPS = 1e-06
MESH = pl.DeviceIdType.MESH
F32 = jnp.float32
BF16 = jnp.bfloat16
DMA = pltpu.SemaphoreType.DMA


def silu(v):
    return v / (1.0 + jnp.exp(-v))


def dot(a, b):
    return jnp.dot(a, b, preferred_element_type=F32)


def dot_t(a, b, precision=None):
    return lax.dot_general(a, b, (((1,), (1,)), ((), ())), precision=precision,
                           preferred_element_type=F32)


def far_first(n):
    return sorted(range(1, n), key=lambda d: -min(d, n - d))


def remote(src, dst, send, recv, where):
    return pltpu.make_async_remote_copy(
        src_ref=src, dst_ref=dst, send_sem=send, recv_sem=recv,
        device_id=where, device_id_type=MESH,
    )


class Place:
    def __init__(self, nk, nt):
        self.nk, self.nt, self.nx = nk, nt, nt // 2
        self.kv, self.tp = lax.axis_index("kv"), lax.axis_index("tp")
        self.core = lax.rem(self.tp, 2)
        self.x = lax.div(self.tp, 2)
        self.partner = {"tp": self.tp + 1 - 2 * self.core}

    def kv_to(self, d):
        return lax.rem(self.kv + d, self.nk)

    def kv_from(self, d):
        return lax.rem(self.kv + self.nk - d, self.nk)

    def tp_to(self, d):
        return lax.rem(self.tp + d, self.nt)

    def tp_from(self, d):
        return lax.rem(self.tp + self.nt - d, self.nt)

    def x_to(self, e):
        return lax.rem(self.x + e, self.nx)

    def x_from(self, e):
        return lax.rem(self.x + self.nx - e, self.nx)

    def same_core(self, x):
        return {"tp": 2 * x + self.core}

    def cross_core(self, x):
        return {"tp": 2 * x + 1 - self.core}


def enter(p):
    barrier = pltpu.get_barrier_semaphore()
    for d in range(1, p.nk):
        pl.semaphore_signal(barrier, inc=1, device_id={"kv": p.kv_to(d)}, device_id_type=MESH)
    for d in range(1, p.nt):
        pl.semaphore_signal(barrier, inc=1, device_id={"tp": p.tp_to(d)}, device_id_type=MESH)
    pl.semaphore_wait(barrier, p.nk + p.nt - 2)


def half_scratch(nk, nt, rows, width, halfc):
    total, nx = nk * rows, nt // 2
    chunks, size = nk // nx, rows
    vmem = pltpu.VMEM
    return dict(
        wg=vmem((2, halfc, width), BF16), wu=vmem((2, halfc, width), BF16),
        wd=vmem((2, halfc, width), BF16), wl=DMA((4,)), ws=DMA((2,)), wr=DMA((2,)),
        xall=vmem((total, width), BF16), xg=vmem((2, total, width), BF16),
        sq=vmem((nx, chunks, 8, size), F32), sqr=vmem((nt, chunks, 8, size), F32),
        part=vmem((nx, chunks, 2, size, halfc), BF16),
        parr=vmem((nx, chunks, 2, size, halfc), BF16),
        mine=vmem((2, nk // nx * rows, halfc), F32),
        hid=vmem((2, total, halfc), BF16),
        dpart=vmem((total, width), BF16), dparr=vmem((nk, rows, width), BF16),
        ag_s=DMA((nk,)), ag_r=DMA((nk,)), dd_s=DMA((nk,)), dd_r=DMA((nk,)),
        sq_s=DMA((nt, chunks)), sq_r=DMA((nt, chunks)),
        rs_s=DMA((nx, chunks)), rs_r=DMA((nx, chunks)),
        hx_s=DMA((nx, 2, chunks)), hx_r=DMA((nx, 2, chunks)),
        dn_s=DMA((nk,)), dn_r=DMA((nk,)),
    )


def local_weights(p, s, gate, lift, down):
    copies = [
        pltpu.make_async_copy(gate.at[p.core], s["wg"].at[0], s["wl"].at[0]),
        pltpu.make_async_copy(lift.at[p.core], s["wu"].at[0], s["wl"].at[1]),
        pltpu.make_async_copy(down.at[p.core], s["wd"].at[0], s["wl"].at[2]),
        pltpu.make_async_copy(down.at[1 - p.core], s["wd"].at[1], s["wl"].at[3]),
    ]
    for c in copies:
        c.start()
    return copies


def swap_weights(p, s, gate, lift):
    copies = [
        remote(gate.at[1 - p.core], s["wg"].at[1], s["ws"].at[0], s["wr"].at[0], p.partner),
        remote(lift.at[1 - p.core], s["wu"].at[1], s["ws"].at[1], s["wr"].at[1], p.partner),
    ]
    for c in copies:
        c.start()
    return copies


def flip_bits(v, m):
    out, bit = v, 1
    while bit <= m:
        if m & bit:
            out = out + bit * (1 - 2 * lax.rem(lax.div(v, bit), 2))
        bit *= 2
    return out


def half_step(p, s, x_ref, gain, local, swapped, idle, tag=''):
    nk, nt, nx = p.nk, p.nt, p.nx
    rows, width = x_ref.shape
    per = nk // nx
    chunks, size = per, rows
    features = width * nt
    near = lax.div(p.kv, nx)
    order = [flip_bits(near, i) for i in range(chunks)]
    peers = far_first(nx)
    sends = []

    def block(k):
        spot = lax.rem(k, nx) * per + lax.div(k, nx)
        return pl.ds(pl.multiple_of(spot * rows, rows), rows)

    def chunk(x, i):
        return pl.ds(pl.multiple_of((x * per + order[i]) * rows, size), size)

    def member(x, i):
        return order[i] * nx + x
    for m in range(1, nk):
        c = remote(x_ref, s["xall"].at[block(p.kv)], s["ag_s"].at[m], s["ag_r"].at[p.kv],
                   {"kv": flip_bits(p.kv, m)})
        c.start()
        sends.append(c)
    s["xall"][block(p.kv), :] = x_ref[...]
    idle[0]()

    def landed(ref, sem):
        pltpu.make_async_copy(ref, ref, sem).wait()

    def arrive(k):
        at = block(k)

        @pl.when(k != p.kv)
        def _():
            landed(s["xall"].at[at], s["ag_r"].at[k])

        value = s["xall"][at, :].astype(F32)
        s["xg"][0, at, :] = (value * gain).astype(BF16)
        remote(s["xg"].at[0, at], s["xg"].at[1, at], s["dd_s"].at[k], s["dd_r"].at[k],
               p.partner).start()
        value = value * value
        folded = value[:, :128]
        for i in range(128, width, 128):
            folded = folded + value[:, i:i + 128]
        return jnp.broadcast_to(jnp.sum(jnp.transpose(folded), axis=0, keepdims=True), (8, rows))

    def ready(k):
        landed(s["xg"].at[1, block(k)], s["dd_r"].at[k])

    squares, parts = {}, {}

    def collect(i):
        for e in peers + [0]:
            to = p.x_to(e)
            s["sq"][e, i] = arrive(member(to, i))
            for other in range(2):
                if e or other:
                    where = p.same_core(to) if not other else p.cross_core(to)
                    c = remote(s["sq"].at[e, i], s["sqr"].at[2 * e + other, i],
                               s["sq_s"].at[2 * e + other, i], s["sq_r"].at[2 * e + other, i],
                               where)
                    c.start()
                    squares[2 * e + other, i] = c
    collect(0)
    for i in range(chunks):
        if i + 1 < chunks:
            collect(i + 1)
        if i == 0:
            local[0].wait()
            local[1].wait()
            for c in swapped:
                c.wait_recv()
        for e in peers:
            to = p.x_to(e)
            ready(member(to, i))
            at = chunk(to, i)
            for j, w in enumerate((s["wg"], s["wu"])):
                s["part"][e, i, j] = (dot_t(s["xg"][0, at, :], w[0])
                                      + dot_t(s["xg"][1, at, :], w[1])).astype(BF16)
            c = remote(s["part"].at[e, i], s["parr"].at[e, i], s["rs_s"].at[e, i],
                       s["rs_r"].at[e, i], p.same_core(to))
            c.start()
            parts[e, i] = c
    for i in range(chunks):
        ready(member(p.x, i))
    whole = pl.ds(pl.multiple_of(p.x * per * rows, rows), per * rows)
    for j, w in enumerate((s["wg"], s["wu"])):
        s["mine"][j] = dot_t(s["xg"][0, whole, :], w[0]) + dot_t(s["xg"][1, whole, :], w[1])
    sends += list(squares.values()) + list(parts.values())
    idle[1]()
    spread = {}
    for i in range(chunks):
        sq = s["sq"][0, i]
        for n in range(1, nt):
            squares[n, i].wait_recv()
            sq = sq + s["sqr"][n, i]
        factor = jnp.transpose(lax.rsqrt(sq / features + EPS))[:, :1]
        own = pl.ds(pl.multiple_of(order[i] * rows, rows), rows)
        gate, lift = s["mine"][0, own, :], s["mine"][1, own, :]
        for e in reversed(peers):
            parts[e, i].wait_recv()
            gate = gate + s["parr"][e, i, 0].astype(F32)
            lift = lift + s["parr"][e, i, 1].astype(F32)
        at = chunk(p.x, i)
        s["hid"][0, at, :] = (silu(gate * factor) * (lift * factor)).astype(BF16)
        for e in peers + [0]:
            for other in range(2):
                if e or other:
                    to = p.x_to(e)
                    where = p.same_core(to) if not other else p.cross_core(to)
                    c = remote(s["hid"].at[0, at], s["hid"].at[other, at],
                               s["hx_s"].at[e, other, i], s["hx_r"].at[e, other, i], where)
                    c.start()
                    spread[e, other, i] = c
    sends += spread.values()
    idle[2]()
    local[2].wait()
    local[3].wait()
    for e in [0] + list(reversed(peers)):
        source = p.x_from(e)
        for i in range(chunks):
            at = chunk(source, i)
            if e:
                spread[e, 0, i].wait_recv()
            spread[e, 1, i].wait_recv()
            mid = dot(s["hid"][0, at, :], s["wd"][0]) + dot(s["hid"][1, at, :], s["wd"][1])
            s["dpart"][at, :] = mid.astype(BF16)
            to = member(source, i)

            @pl.when(to != p.kv)
            def _():
                remote(s["dpart"].at[block(to)], s["dparr"].at[p.kv], s["dn_s"].at[to],
                       s["dn_r"].at[p.kv], {"kv": to}).start()
    idle[3]()
    acc = s["dpart"][block(p.kv), :].astype(F32)
    for m in range(1, nk):
        source = flip_bits(p.kv, m)
        landed(s["dparr"].at[source], s["dn_r"].at[source])
        acc = acc + s["dparr"][source].astype(F32)
    def finish():
        for m in range(1, nk):
            to = flip_bits(p.kv, m)
            landed(s["dparr"].at[to], s["dn_s"].at[to])
        for k in range(nk):
            landed(s["xg"].at[1, block(k)], s["dd_s"].at[k])
        for c in sends + swapped:
            c.wait_send()

    return x_ref[...].astype(F32) + 0.5 * acc, finish


def conv(taps_ref, buf_ref, newest):
    taps = taps_ref[...].astype(F32)
    count = taps.shape[0]
    old = buf_ref[...].astype(F32)
    acc = newest.astype(BF16).astype(F32) * taps[count - 1:count]
    for k in range(count - 1):
        acc = acc + old[k] * taps[k:k + 1]
    return silu(acc)


def split(v):
    high = v.astype(BF16).astype(F32)
    return high, v - high


def layer_kernel(nk, nt, names, small, *refs):
    tag = 'k_'
    r = dict(zip(names, refs))
    p = Place(nk, nt)
    one = {k[2:]: v for k, v in r.items() if k.startswith("1.")}
    two = {k[2:]: v for k, v in r.items() if k.startswith("2.")}
    state = r["state_out"]
    smalls = {}
    for i, name in enumerate(small):
        smalls[name] = pltpu.make_async_copy(r[name], r["v." + name], r["sl"].at[i])
        smalls[name].start()
        r[name] = r["v." + name]
    x_ref = r["x"]
    rows, width = x_ref.shape
    features = nt * width
    chans = r["wx"].shape[-1]
    gs = r["wb"].shape[-1]
    heads = r["ws"].shape[0]
    groups = gs // STATE
    gch = chans // groups
    hg = heads // groups
    wcat = r["wcat"]
    local1 = local_weights(p, one, r["gate1"], r["lift1"], r["down1"])
    mixload = []
    at = 0
    for i, name in enumerate(("wz", "wx", "wb", "wr")):
        w = r[name]
        c = pltpu.make_async_copy(w, wcat.at[:, :, at:at + w.shape[-1]], r["ml"].at[i])
        at += w.shape[-1]
        mixload.append(c)
    mixload.append(pltpu.make_async_copy(r["wo"], r["wov"], r["ml"].at[4]))
    stateload = pltpu.make_async_copy(r["state"], state, r["ml"].at[5])
    enter(p)
    smalls["x"].wait()
    smalls["g1"].wait()
    swap1 = swap_weights(p, one, r["gate1"], r["lift1"])

    def row(name):
        return r[name][...].astype(F32).reshape(1, -1)

    later = {}

    def load_rest():
        stateload.start()
        for c in mixload:
            c.start()
        later["local"] = local_weights(p, two, r["gate2"], r["lift2"], r["down2"])
        later["swap"] = swap_weights(p, two, r["gate2"], r["lift2"])

    def narrow():
        stateload.wait()

        def body(i, _):
            for g in range(groups):
                pair = [state[2 * i + j, g * hg:(g + 1) * hg].reshape(gch, STATE)
                        for j in range(2)]
                r["stb"][i, g * gch:(g + 1) * gch, :] = jnp.concatenate(pair, axis=1).astype(BF16)
            return 0

        lax.fori_loop(0, rows // 2, body, 0)

    def nothing():
        pass

    first, finish1 = half_step(p, one, x_ref, row("g1"), local1, swap1,
                               (load_rest, narrow, nothing, nothing), 'a_')
    held = r["held"]
    held[p.tp] = first.astype(BF16)
    copies = {}
    for d in far_first(nt):
        c = remote(held.at[p.tp], held.at[p.tp], r["f_s"].at[d], r["f_r"].at[d],
                   {"tp": p.tp_to(d)})
        c.start()
        copies[d] = c
    for c in mixload:
        c.wait()
    for name in small[2:]:
        smalls[name].wait()
    gm = row("gm")
    gmv = r["gmv"]
    for t in range(nt):
        gmv[t] = gm[:, t * width:(t + 1) * width]
    total = jnp.zeros((rows, 1), F32)
    proj = jnp.zeros((rows, wcat.shape[-1]), F32)
    raw = jnp.zeros((rows, heads), F32)
    for d in [0] + list(reversed(far_first(nt))):
        t = p.tp_from(d)
        if d:
            copies[d].wait_recv()
        v = held[t].astype(F32)
        total = total + jnp.sum(v * v, axis=1, keepdims=True)
        scaled = (v * gmv[t]).astype(BF16)
        proj = proj + dot(scaled, wcat[t])
        raw = raw + dot_t(scaled, r["ws"][:, pl.ds(pl.multiple_of(t * width, width), width)])
    factor = lax.rsqrt(total / features + EPS)
    proj = proj * factor
    raw = (raw * factor).astype(BF16).astype(F32) + r["bias"][...]

    def spread(v):
        a = lax.broadcasted_iota(jnp.int32, (heads, chans), 0)
        c = lax.broadcasted_iota(jnp.int32, (heads, chans), 1)
        ind = jnp.where(c // HEAD_DIM == a, 1.0, 0.0).astype(F32)
        return jnp.dot(v, ind, precision=lax.Precision.HIGHEST, preferred_element_type=F32)

    z = proj[:, :chans].astype(BF16).astype(F32)
    xc = conv(r["tx"], r["bx"], proj[:, chans:2 * chans])
    bc = conv(r["tb"], r["bb"], proj[:, 2 * chans:2 * chans + gs])
    rc = conv(r["tr"], r["br"], proj[:, 2 * chans + gs:])
    step = jnp.maximum(raw, 0.0) + jnp.log1p(jnp.exp(-jnp.abs(raw)))
    retain = jnp.exp(-step * jnp.exp(r["rate"][...]))
    sx = spread(step) * xc
    keep = spread(retain)
    rowid = lax.broadcasted_iota(jnp.int32, (rows, 2 * STATE), 0)
    colid = lax.broadcasted_iota(jnp.int32, (rows, 2 * STATE), 1) // STATE
    pieces = []
    for g in range(groups):
        rg = rc[:, g * STATE:(g + 1) * STATE]
        twice = jnp.concatenate([rg, rg], axis=1)
        acc = jnp.zeros((rows, gch), F32)
        for i in range(rows // 2):
            lhs = jnp.where(rowid - colid == 2 * i, twice, 0.0).astype(BF16)
            acc = acc + dot_t(lhs, r["stb"][i, g * gch:(g + 1) * gch, :])
        br = jnp.sum(bc[:, g * STATE:(g + 1) * STATE] * rg, axis=1, keepdims=True)
        pieces.append(acc * keep[:, g * gch:(g + 1) * gch] + sx[:, g * gch:(g + 1) * gch] * br)
    out = jnp.concatenate(pieces, axis=1) + spread(r["skip"][...]) * xc
    gated = out.astype(BF16).astype(F32) * silu(z)
    pieces = []
    for g in range(groups):
        v = gated[:, g * gch:(g + 1) * gch]
        pieces.append(v * lax.rsqrt(jnp.mean(v * v, axis=1, keepdims=True) + EPS))
    gated = (jnp.concatenate(pieces, axis=1) * row("gg")).astype(BF16)
    pout, arrived = r["pout"], r["arrived"]
    outs = {}
    for d in far_first(nt) + [0]:
        to = p.tp_to(d)
        wo = r["wov"][:, pl.ds(pl.multiple_of(to * width, width), width)]
        pout[d] = dot(gated, wo).astype(BF16)
        if d:
            c = remote(pout.at[d], arrived.at[d], r["m_s"].at[d], r["m_r"].at[d], {"tp": to})
            c.start()
            outs[d] = c
    depth = r["base"].shape[1]
    pad = depth - 5 * rows
    sx_hi, sx_lo = split(sx)
    re_hi, re_lo = split(keep)
    left = jnp.concatenate(
        [sx_hi, sx_lo, sx_hi, re_hi, re_lo, jnp.zeros((pad, chans), F32)], axis=0)
    r["left"][...] = left.T.astype(BF16)
    for g in range(groups):
        b_hi, b_lo = split(bc[:, g * STATE:(g + 1) * STATE])
        zero = jnp.zeros((rows, STATE), F32)
        full = jnp.ones((rows, STATE), F32)
        zpad = jnp.zeros((pad, STATE), F32)
        r["base"][g, :, :STATE] = jnp.concatenate(
            [b_hi, b_hi, b_lo, zero, zero, zpad], axis=0).astype(BF16)
        r["base"][g, :, STATE:] = jnp.concatenate(
            [zero, zero, zero, full, full, zpad], axis=0).astype(BF16)
    acc = held[p.tp].astype(F32) + pout[0].astype(F32)
    for d in reversed(far_first(nt)):
        outs[d].wait_recv()
        acc = acc + arrived[d].astype(F32)
    r["mixed"][...] = acc.astype(BF16)

    rowmod = lax.rem(lax.broadcasted_iota(jnp.int32, (depth, 2 * STATE), 0), rows)

    def update(low, high):
        def body(b, _):
            mask = jnp.where(rowmod == b, 1.0, 0.0).astype(BF16)
            for g in range(groups):
                right = r["base"][g] * mask
                both = dot(r["left"][g * gch:(g + 1) * gch, :], right)
                old = state[b, g * hg:(g + 1) * hg].reshape(gch, STATE)
                new = both[:, STATE:] * old + both[:, :STATE]
                state[b, g * hg:(g + 1) * hg] = new.reshape(hg, HEAD_DIM, STATE)
            return 0

        return lambda: lax.fori_loop(low, high, body, 0)

    cuts = (rows * 3 // 8, rows * 5 // 8)
    last, finish2 = half_step(p, two, r["mixed"], row("g2"), later["local"], later["swap"],
                              (update(0, cuts[0]), nothing, update(cuts[0], cuts[1]),
                               update(cuts[1], rows)), 'b_')
    r["out"][...] = last.astype(BF16)
    finish1()
    finish2()
    for c in list(copies.values()) + list(outs.values()):
        c.wait_send()


def flush_kernel(a, b, oa, ob, sem):
    pieces = sem.shape[0] - 1
    step = b.shape[0] // pieces
    copies = [pltpu.make_async_copy(a, oa, sem.at[pieces])]
    for i in range(pieces):
        at = pl.ds(i * step, step)
        copies.append(pltpu.make_async_copy(b.at[at], ob.at[at], sem.at[i]))
    for c in copies:
        c.start()
    for c in copies:
        c.wait()


def per_device(nk, nt, residual, first_gain, first_gate, first_lift, first_down,
               mixer_gain, wz, wx, wb, wr, ws, bias, rate, skip, tx, tb, tr, bx, bb, br,
               state, group_gain, wo, second_gain, second_gate, second_lift, second_down):
    rows, width = residual.shape
    halfc = first_gate.shape[1] // 2
    chans, heads = wx.shape[1], ws.shape[1]
    groups = wb.shape[1] // STATE
    vmem = pltpu.VMEM

    def tall(w):
        return w.T.reshape(2, halfc, width)

    def flip(v):
        return jnp.transpose(v, (1, 0, 2))

    small = dict(x=residual, g1=first_gain, g2=second_gain, gm=mixer_gain, gg=group_gain,
                 ws=ws.T, bias=bias[None, :], rate=rate[None, :], skip=skip[None, :],
                 tx=tx, tb=tb, tr=tr, bx=flip(bx), bb=flip(bb), br=flip(br))
    big = dict(gate1=tall(first_gate), lift1=tall(first_lift),
               down1=first_down.reshape(2, halfc, width),
               gate2=tall(second_gate), lift2=tall(second_lift),
               down2=second_down.reshape(2, halfc, width),
               wz=wz.reshape(nt, width, -1), wx=wx.reshape(nt, width, -1),
               wb=wb.reshape(nt, width, -1), wr=wr.reshape(nt, width, -1), wo=wo, state=state)
    depth = -(-5 * rows // 128) * 128
    scratch = dict(
        wcat=vmem((nt, width, 2 * chans + 2 * groups * STATE), BF16),
        wov=vmem(wo.shape, BF16), ml=DMA((6,)),
        stb=vmem((rows // 2, chans, 2 * STATE), BF16),
        held=vmem((nt, rows, width), BF16), f_s=DMA((nt,)), f_r=DMA((nt,)),
        gmv=vmem((nt, 1, width), F32),
        pout=vmem((nt, rows, width), BF16), arrived=vmem((nt, rows, width), BF16),
        m_s=DMA((nt,)), m_r=DMA((nt,)), mixed=vmem((rows, width), BF16),
        left=vmem((chans, depth), BF16), base=vmem((groups, depth, 2 * STATE), BF16),
    )
    scratch["sl"] = DMA((len(small),))
    for k, v in small.items():
        scratch["v." + k] = vmem(v.shape, v.dtype)
    for tag in ("1.", "2."):
        for k, v in half_scratch(nk, nt, rows, width, halfc).items():
            scratch[tag + k] = v
    names = list(small) + list(big) + ["out", "state_out"] + list(scratch)
    inside = pl.BlockSpec(memory_space=pltpu.VMEM)
    outside = pl.BlockSpec(memory_space=pl.ANY)
    out, state_out = pl.pallas_call(
        functools.partial(layer_kernel, nk, nt, names, list(small)),
        out_shape=(vmem(residual.shape, BF16), vmem(state.shape, F32)),
        in_specs=[outside] * (len(small) + len(big)),
        out_specs=(inside, inside),
        scratch_shapes=list(scratch.values()),
        compiler_params=pltpu.CompilerParams(
            collective_id=1, has_side_effects=True, vmem_limit_bytes=48 * 1024 * 1024),
        name="layer",
    )(*small.values(), *big.values())
    return pl.pallas_call(
        flush_kernel,
        out_shape=(jax.ShapeDtypeStruct(residual.shape, BF16),
                   jax.ShapeDtypeStruct(state.shape, F32)),
        in_specs=[inside] * 2,
        out_specs=(outside, outside),
        scratch_shapes=[DMA((9,))],
        compiler_params=pltpu.CompilerParams(vmem_limit_bytes=1024 * 1024),
        name="flush",
    )(out, state_out)


def solution(mesh):
    placed = (
        P("kv", "tp"),
        P("tp"),
        P("tp", "kv"),
        P("tp", "kv"),
        P("kv", "tp"),
        P(),
        P(None, "tp"),
        P(None, "tp"),
        P(None, "tp"),
        P(None, "tp"),
        P(None, "tp"),
        P("tp"),
        P("tp"),
        P("tp"),
        P(None, "tp"),
        P(None, "tp"),
        P(None, "tp"),
        P("kv", None, "tp"),
        P("kv", None, "tp"),
        P("kv", None, "tp"),
        P("kv", "tp", None, None),
        P("tp"),
        P("tp", None),
        P("tp"),
        P("tp", "kv"),
        P("tp", "kv"),
        P("kv", "tp"),
    )
    return jax.shard_map(
        functools.partial(per_device, mesh.shape["kv"], mesh.shape["tp"]),
        mesh=mesh,
        in_specs=placed,
        out_specs=(P("kv", "tp"), P("kv", "tp", None, None)),
        check_vma=False,
    )
```

```python
import functools

import jax
import jax.numpy as jnp
from jax import lax
from jax.experimental import pallas as pl
from jax.experimental.pallas import tpu as pltpu
from jax.sharding import PartitionSpec as P

HEAD_DIM = 64
STATE = 128
EPS = 1e-06
MESH = pl.DeviceIdType.MESH
F32 = jnp.float32
BF16 = jnp.bfloat16
DMA = pltpu.SemaphoreType.DMA


def silu(v):
    return v / (1.0 + jnp.exp(-v))


def dot(a, b):
    return jnp.dot(a, b, preferred_element_type=F32)


def dot_t(a, b, precision=None):
    return lax.dot_general(a, b, (((1,), (1,)), ((), ())), precision=precision,
                           preferred_element_type=F32)


def far_first(n):
    return sorted(range(1, n), key=lambda d: -min(d, n - d))


def remote(src, dst, send, recv, where):
    return pltpu.make_async_remote_copy(
        src_ref=src, dst_ref=dst, send_sem=send, recv_sem=recv,
        device_id=where, device_id_type=MESH,
    )


class Place:
    def __init__(self, nk, nt):
        self.nk, self.nt, self.nx = nk, nt, nt // 2
        self.kv, self.tp = lax.axis_index("kv"), lax.axis_index("tp")
        self.core = lax.rem(self.tp, 2)
        self.x = lax.div(self.tp, 2)
        self.partner = {"tp": self.tp + 1 - 2 * self.core}

    def kv_to(self, d):
        return lax.rem(self.kv + d, self.nk)

    def kv_from(self, d):
        return lax.rem(self.kv + self.nk - d, self.nk)

    def tp_to(self, d):
        return lax.rem(self.tp + d, self.nt)

    def tp_from(self, d):
        return lax.rem(self.tp + self.nt - d, self.nt)

    def x_to(self, e):
        return lax.rem(self.x + e, self.nx)

    def x_from(self, e):
        return lax.rem(self.x + self.nx - e, self.nx)

    def same_core(self, x):
        return {"tp": 2 * x + self.core}

    def cross_core(self, x):
        return {"tp": 2 * x + 1 - self.core}


def enter(p):
    barrier = pltpu.get_barrier_semaphore()
    for d in range(1, p.nk):
        pl.semaphore_signal(barrier, inc=1, device_id={"kv": p.kv_to(d)}, device_id_type=MESH)
    for d in range(1, p.nt):
        pl.semaphore_signal(barrier, inc=1, device_id={"tp": p.tp_to(d)}, device_id_type=MESH)
    pl.semaphore_wait(barrier, p.nk + p.nt - 2)


def half_scratch(nk, nt, rows, width, halfc):
    total, nx = nk * rows, nt // 2
    chunks, size = nk // nx, rows
    vmem = pltpu.VMEM
    return dict(
        wg=vmem((2, halfc, width), BF16), wu=vmem((2, halfc, width), BF16),
        wd=vmem((2, halfc, width), BF16), wl=DMA((4,)), ws=DMA((2,)), wr=DMA((2,)),
        xall=vmem((total, width), BF16), xg=vmem((2, total, width), BF16),
        sq=vmem((nx, chunks, 8, size), F32), sqr=vmem((nt, chunks, 8, size), F32),
        part=vmem((nx, chunks, 2, size, halfc), BF16),
        parr=vmem((nx, chunks, 2, size, halfc), BF16),
        mine=vmem((2, nk // nx * rows, halfc), F32),
        hid=vmem((2, total, halfc), BF16),
        dpart=vmem((total, width), BF16), dparr=vmem((nk, rows, width), BF16),
        ag_s=DMA((nk,)), ag_r=DMA((nk,)), dd_s=DMA((nk,)), dd_r=DMA((nk,)),
        sq_s=DMA((nt, chunks)), sq_r=DMA((nt, chunks)),
        rs_s=DMA((nx, chunks)), rs_r=DMA((nx, chunks)),
        hx_s=DMA((nx, 2, chunks)), hx_r=DMA((nx, 2, chunks)),
        dn_s=DMA((nk,)), dn_r=DMA((nk,)),
    )


def local_weights(p, s, gate, lift, down):
    copies = [
        pltpu.make_async_copy(gate.at[p.core], s["wg"].at[0], s["wl"].at[0]),
        pltpu.make_async_copy(lift.at[p.core], s["wu"].at[0], s["wl"].at[1]),
        pltpu.make_async_copy(down.at[p.core], s["wd"].at[0], s["wl"].at[2]),
        pltpu.make_async_copy(down.at[1 - p.core], s["wd"].at[1], s["wl"].at[3]),
    ]
    for c in copies:
        c.start()
    return copies


def swap_weights(p, s, gate, lift):
    copies = [
        remote(gate.at[1 - p.core], s["wg"].at[1], s["ws"].at[0], s["wr"].at[0], p.partner),
        remote(lift.at[1 - p.core], s["wu"].at[1], s["ws"].at[1], s["wr"].at[1], p.partner),
    ]
    for c in copies:
        c.start()
    return copies


def flip_bits(v, m):
    out, bit = v, 1
    while bit <= m:
        if m & bit:
            out = out + bit * (1 - 2 * lax.rem(lax.div(v, bit), 2))
        bit *= 2
    return out


def half_step(p, s, x_ref, gain, local, swapped, idle, tag=''):
    nk, nt, nx = p.nk, p.nt, p.nx
    rows, width = x_ref.shape
    per = nk // nx
    chunks, size = per, rows
    features = width * nt
    near = lax.div(p.kv, nx)
    order = [flip_bits(near, i) for i in range(chunks)]
    peers = far_first(nx)
    sends = []

    def block(k):
        spot = lax.rem(k, nx) * per + lax.div(k, nx)
        return pl.ds(pl.multiple_of(spot * rows, rows), rows)

    def chunk(x, i):
        return pl.ds(pl.multiple_of((x * per + order[i]) * rows, size), size)

    def member(x, i):
        return order[i] * nx + x
    for m in range(1, nk):
        c = remote(x_ref, s["xall"].at[block(p.kv)], s["ag_s"].at[m], s["ag_r"].at[p.kv],
                   {"kv": flip_bits(p.kv, m)})
        c.start()
        sends.append(c)
    s["xall"][block(p.kv), :] = x_ref[...]
    idle[0]()

    def landed(ref, sem):
        pltpu.make_async_copy(ref, ref, sem).wait()

    def arrive(k):
        at = block(k)

        @pl.when(k != p.kv)
        def _():
            landed(s["xall"].at[at], s["ag_r"].at[k])

        value = s["xall"][at, :].astype(F32)
        s["xg"][0, at, :] = (value * gain).astype(BF16)
        remote(s["xg"].at[0, at], s["xg"].at[1, at], s["dd_s"].at[k], s["dd_r"].at[k],
               p.partner).start()
        value = value * value
        folded = value[:, :128]
        for i in range(128, width, 128):
            folded = folded + value[:, i:i + 128]
        return jnp.broadcast_to(jnp.sum(jnp.transpose(folded), axis=0, keepdims=True), (8, rows))

    def ready(k):
        landed(s["xg"].at[1, block(k)], s["dd_r"].at[k])

    squares, parts = {}, {}

    def collect(i):
        for e in peers + [0]:
            to = p.x_to(e)
            s["sq"][e, i] = arrive(member(to, i))
            for other in range(2):
                if e or other:
                    where = p.same_core(to) if not other else p.cross_core(to)
                    c = remote(s["sq"].at[e, i], s["sqr"].at[2 * e + other, i],
                               s["sq_s"].at[2 * e + other, i], s["sq_r"].at[2 * e + other, i],
                               where)
                    c.start()
                    squares[2 * e + other, i] = c
    collect(0)
    for i in range(chunks):
        if i + 1 < chunks:
            collect(i + 1)
        if i == 0:
            local[0].wait()
            local[1].wait()
            for c in swapped:
                c.wait_recv()
        for e in peers:
            to = p.x_to(e)
            ready(member(to, i))
            at = chunk(to, i)
            for j, w in enumerate((s["wg"], s["wu"])):
                s["part"][e, i, j] = (dot_t(s["xg"][0, at, :], w[0])
                                      + dot_t(s["xg"][1, at, :], w[1])).astype(BF16)
            c = remote(s["part"].at[e, i], s["parr"].at[e, i], s["rs_s"].at[e, i],
                       s["rs_r"].at[e, i], p.same_core(to))
            c.start()
            parts[e, i] = c
    for i in range(chunks):
        ready(member(p.x, i))
    whole = pl.ds(pl.multiple_of(p.x * per * rows, rows), per * rows)
    for j, w in enumerate((s["wg"], s["wu"])):
        s["mine"][j] = dot_t(s["xg"][0, whole, :], w[0]) + dot_t(s["xg"][1, whole, :], w[1])
    sends += list(squares.values()) + list(parts.values())
    idle[1]()
    spread = {}
    for i in range(chunks):
        sq = s["sq"][0, i]
        for n in range(1, nt):
            squares[n, i].wait_recv()
            sq = sq + s["sqr"][n, i]
        factor = jnp.transpose(lax.rsqrt(sq / features + EPS))[:, :1]
        own = pl.ds(pl.multiple_of(order[i] * rows, rows), rows)
        gate, lift = s["mine"][0, own, :], s["mine"][1, own, :]
        for e in reversed(peers):
            parts[e, i].wait_recv()
            gate = gate + s["parr"][e, i, 0].astype(F32)
            lift = lift + s["parr"][e, i, 1].astype(F32)
        at = chunk(p.x, i)
        s["hid"][0, at, :] = (silu(gate * factor) * (lift * factor)).astype(BF16)
        for e in peers + [0]:
            for other in range(2):
                if e or other:
                    to = p.x_to(e)
                    where = p.same_core(to) if not other else p.cross_core(to)
                    c = remote(s["hid"].at[0, at], s["hid"].at[other, at],
                               s["hx_s"].at[e, other, i], s["hx_r"].at[e, other, i], where)
                    c.start()
                    spread[e, other, i] = c
    sends += spread.values()
    local[2].wait()
    local[3].wait()
    for e in [0] + list(reversed(peers)):
        source = p.x_from(e)
        if e == (peers or [0])[-1]:
            idle[2]()
        for i in range(chunks):
            at = chunk(source, i)
            if e:
                spread[e, 0, i].wait_recv()
            spread[e, 1, i].wait_recv()
            mid = dot(s["hid"][0, at, :], s["wd"][0]) + dot(s["hid"][1, at, :], s["wd"][1])
            s["dpart"][at, :] = mid.astype(BF16)
            to = member(source, i)

            @pl.when(to != p.kv)
            def _():
                remote(s["dpart"].at[block(to)], s["dparr"].at[p.kv], s["dn_s"].at[to],
                       s["dn_r"].at[p.kv], {"kv": to}).start()
    idle[3]()
    acc = s["dpart"][block(p.kv), :].astype(F32)
    for m in range(1, nk):
        source = flip_bits(p.kv, m)
        landed(s["dparr"].at[source], s["dn_r"].at[source])
        acc = acc + s["dparr"][source].astype(F32)
    def finish():
        for m in range(1, nk):
            to = flip_bits(p.kv, m)
            landed(s["dparr"].at[to], s["dn_s"].at[to])
        for k in range(nk):
            landed(s["xg"].at[1, block(k)], s["dd_s"].at[k])
        for c in sends + swapped:
            c.wait_send()

    return x_ref[...].astype(F32) + 0.5 * acc, finish


def conv(taps_ref, buf_ref, newest):
    taps = taps_ref[...].astype(F32)
    count = taps.shape[0]
    old = buf_ref[...].astype(F32)
    acc = newest.astype(BF16).astype(F32) * taps[count - 1:count]
    for k in range(count - 1):
        acc = acc + old[k] * taps[k:k + 1]
    return silu(acc)


def split(v):
    high = v.astype(BF16).astype(F32)
    return high, v - high


def layer_kernel(nk, nt, names, small, *refs):
    tag = 'k_'
    r = dict(zip(names, refs))
    p = Place(nk, nt)
    one = {k[2:]: v for k, v in r.items() if k.startswith("1.")}
    two = {k[2:]: v for k, v in r.items() if k.startswith("2.")}
    state = r["state_out"]
    smalls = {}
    for i, name in enumerate(small):
        smalls[name] = pltpu.make_async_copy(r[name], r["v." + name], r["sl"].at[i])
        smalls[name].start()
        r[name] = r["v." + name]
    x_ref = r["x"]
    rows, width = x_ref.shape
    features = nt * width
    chans = r["wx"].shape[-1]
    gs = r["wb"].shape[-1]
    heads = r["ws"].shape[0]
    groups = gs // STATE
    gch = chans // groups
    hg = heads // groups
    wcat = r["wcat"]
    local1 = local_weights(p, one, r["gate1"], r["lift1"], r["down1"])
    mixload = []
    at = 0
    for i, name in enumerate(("wz", "wx", "wb", "wr")):
        w = r[name]
        c = pltpu.make_async_copy(w, wcat.at[:, :, at:at + w.shape[-1]], r["ml"].at[i])
        at += w.shape[-1]
        mixload.append(c)
    mixload.append(pltpu.make_async_copy(r["wo"], r["wov"], r["ml"].at[4]))
    stateload = pltpu.make_async_copy(r["state"], state, r["ml"].at[5])
    stateload.start()
    enter(p)
    smalls["x"].wait()
    smalls["g1"].wait()
    swap1 = swap_weights(p, one, r["gate1"], r["lift1"])

    def row(name):
        return r[name][...].astype(F32).reshape(1, -1)

    later = {}

    def load_rest():
        for c in mixload:
            c.start()
        later["local"] = local_weights(p, two, r["gate2"], r["lift2"], r["down2"])
        narrow()

    def narrow():
        stateload.wait()

        def body(i, _):
            for g in range(groups):
                for j in range(2):
                    old = state[2 * i + j, g * hg:(g + 1) * hg].reshape(gch, STATE)
                    r["stb"][i, g, j * STATE:(j + 1) * STATE, :] = jnp.transpose(old).astype(BF16)
            return 0

        lax.fori_loop(0, rows // 2, body, 0)

    def swap_rest():
        later["swap"] = swap_weights(p, two, r["gate2"], r["lift2"])

    def nothing():
        pass

    first, finish1 = half_step(p, one, x_ref, row("g1"), local1, swap1,
                               (load_rest, swap_rest, nothing, nothing), 'a_')
    held = r["held"]
    held[p.tp] = first.astype(BF16)
    copies = {}
    for d in far_first(nt):
        c = remote(held.at[p.tp], held.at[p.tp], r["f_s"].at[d], r["f_r"].at[d],
                   {"tp": p.tp_to(d)})
        c.start()
        copies[d] = c
    for c in mixload:
        c.wait()
    for name in small[2:]:
        smalls[name].wait()
    gm = row("gm")
    gmv = r["gmv"]
    for t in range(nt):
        gmv[t] = gm[:, t * width:(t + 1) * width]
    total = jnp.zeros((rows, 1), F32)
    proj = jnp.zeros((rows, wcat.shape[-1]), F32)
    raw = jnp.zeros((rows, heads), F32)
    for d in [0] + list(reversed(far_first(nt))):
        t = p.tp_from(d)
        if d:
            copies[d].wait_recv()
        v = held[t].astype(F32)
        total = total + jnp.sum(v * v, axis=1, keepdims=True)
        scaled = (v * gmv[t]).astype(BF16)
        proj = proj + dot(scaled, wcat[t])
        raw = raw + dot_t(scaled, r["ws"][:, pl.ds(pl.multiple_of(t * width, width), width)])
    factor = lax.rsqrt(total / features + EPS)
    proj = proj * factor
    raw = (raw * factor).astype(BF16).astype(F32) + r["bias"][...]

    def spread(v):
        a = lax.broadcasted_iota(jnp.int32, (heads, chans), 0)
        c = lax.broadcasted_iota(jnp.int32, (heads, chans), 1)
        ind = jnp.where(c // HEAD_DIM == a, 1.0, 0.0).astype(F32)
        return jnp.dot(v, ind, precision=lax.Precision.HIGHEST, preferred_element_type=F32)

    z = proj[:, :chans].astype(BF16).astype(F32)
    xc = conv(r["tx"], r["bx"], proj[:, chans:2 * chans])
    bc = conv(r["tb"], r["bb"], proj[:, 2 * chans:2 * chans + gs])
    rc = conv(r["tr"], r["br"], proj[:, 2 * chans + gs:])
    step = jnp.maximum(raw, 0.0) + jnp.log1p(jnp.exp(-jnp.abs(raw)))
    retain = jnp.exp(-step * jnp.exp(r["rate"][...]))
    sx = spread(step) * xc
    keep = spread(retain)
    rowid = lax.broadcasted_iota(jnp.int32, (rows, 2 * STATE), 0)
    colid = lax.broadcasted_iota(jnp.int32, (rows, 2 * STATE), 1) // STATE
    pieces = []
    for g in range(groups):
        rg = rc[:, g * STATE:(g + 1) * STATE]
        twice = jnp.concatenate([rg, rg], axis=1)
        acc = jnp.zeros((rows, gch), F32)
        for i in range(rows // 2):
            lhs = jnp.where(rowid - colid == 2 * i, twice, 0.0).astype(BF16)
            acc = acc + dot(lhs, r["stb"][i, g])
        br = jnp.sum(bc[:, g * STATE:(g + 1) * STATE] * rg, axis=1, keepdims=True)
        pieces.append(acc * keep[:, g * gch:(g + 1) * gch] + sx[:, g * gch:(g + 1) * gch] * br)
    out = jnp.concatenate(pieces, axis=1) + spread(r["skip"][...]) * xc
    gated = out.astype(BF16).astype(F32) * silu(z)
    pieces = []
    for g in range(groups):
        v = gated[:, g * gch:(g + 1) * gch]
        pieces.append(v * lax.rsqrt(jnp.mean(v * v, axis=1, keepdims=True) + EPS))
    gated = (jnp.concatenate(pieces, axis=1) * row("gg")).astype(BF16)
    pout, arrived = r["pout"], r["arrived"]
    outs = {}
    for d in far_first(nt) + [0]:
        to = p.tp_to(d)
        wo = r["wov"][:, pl.ds(pl.multiple_of(to * width, width), width)]
        pout[d] = dot(gated, wo).astype(BF16)
        if d:
            c = remote(pout.at[d], arrived.at[d], r["m_s"].at[d], r["m_r"].at[d], {"tp": to})
            c.start()
            outs[d] = c
    depth = r["base"].shape[1]
    pad = depth - 3 * rows
    re_hi, re_lo = split(keep)
    left = jnp.concatenate([sx, re_hi, re_lo, jnp.zeros((pad, chans), F32)], axis=0)
    r["left"][...] = left.T.astype(BF16)
    for g in range(groups):
        zero = jnp.zeros((2 * rows + pad, STATE), F32)
        full = jnp.ones((2 * rows, STATE), F32)
        r["base"][g, :, :STATE] = jnp.concatenate(
            [bc[:, g * STATE:(g + 1) * STATE], zero], axis=0).astype(BF16)
        r["base"][g, :, STATE:] = jnp.concatenate(
            [zero[:rows], full, zero[:pad]], axis=0).astype(BF16)
    acc = held[p.tp].astype(F32) + pout[0].astype(F32)
    for d in reversed(far_first(nt)):
        outs[d].wait_recv()
        acc = acc + arrived[d].astype(F32)
    r["mixed"][...] = acc.astype(BF16)

    rowmod = lax.rem(lax.broadcasted_iota(jnp.int32, (depth, 2 * STATE), 0), rows)

    def update(low, high):
        many = 4 if (high - low) % 4 == 0 else 1

        def body(n, _):
            for j in range(many):
                b = low + n * many + j
                mask = jnp.where(rowmod == b, 1.0, 0.0).astype(BF16)
                for g in range(groups):
                    right = r["base"][g] * mask
                    both = dot(r["left"][g * gch:(g + 1) * gch, :], right)
                    old = state[b, g * hg:(g + 1) * hg].reshape(gch, STATE)
                    new = both[:, STATE:] * old + both[:, :STATE]
                    state[b, g * hg:(g + 1) * hg] = new.reshape(hg, HEAD_DIM, STATE)
            return 0

        return lambda: lax.fori_loop(0, (high - low) // many, body, 0)

    cuts = [rows * n // 16 for n in (0, 6, 8, 12, 16)]
    last, finish2 = half_step(p, two, r["mixed"], row("g2"), later["local"], later["swap"],
                              tuple(update(cuts[n], cuts[n + 1]) for n in range(4)), 'b_')
    r["out"][...] = last.astype(BF16)
    finish1()
    finish2()
    for c in list(copies.values()) + list(outs.values()):
        c.wait_send()


def flush_kernel(a, b, oa, ob, sem):
    pieces = sem.shape[0] - 1
    step = b.shape[0] // pieces
    copies = [pltpu.make_async_copy(a, oa, sem.at[pieces])]
    for i in range(pieces):
        at = pl.ds(i * step, step)
        copies.append(pltpu.make_async_copy(b.at[at], ob.at[at], sem.at[i]))
    for c in copies:
        c.start()
    for c in copies:
        c.wait()


def per_device(nk, nt, residual, first_gain, first_gate, first_lift, first_down,
               mixer_gain, wz, wx, wb, wr, ws, bias, rate, skip, tx, tb, tr, bx, bb, br,
               state, group_gain, wo, second_gain, second_gate, second_lift, second_down):
    rows, width = residual.shape
    halfc = first_gate.shape[1] // 2
    chans, heads = wx.shape[1], ws.shape[1]
    groups = wb.shape[1] // STATE
    vmem = pltpu.VMEM

    def tall(w):
        return w.T.reshape(2, halfc, width)

    def flip(v):
        return jnp.transpose(v, (1, 0, 2))

    small = dict(x=residual, g1=first_gain, g2=second_gain, gm=mixer_gain, gg=group_gain,
                 ws=ws.T, bias=bias[None, :], rate=rate[None, :], skip=skip[None, :],
                 tx=tx, tb=tb, tr=tr, bx=flip(bx), bb=flip(bb), br=flip(br))
    big = dict(gate1=tall(first_gate), lift1=tall(first_lift),
               down1=first_down.reshape(2, halfc, width),
               gate2=tall(second_gate), lift2=tall(second_lift),
               down2=second_down.reshape(2, halfc, width),
               wz=wz.reshape(nt, width, -1), wx=wx.reshape(nt, width, -1),
               wb=wb.reshape(nt, width, -1), wr=wr.reshape(nt, width, -1), wo=wo, state=state)
    depth = -(-3 * rows // 128) * 128
    scratch = dict(
        wcat=vmem((nt, width, 2 * chans + 2 * groups * STATE), BF16),
        wov=vmem(wo.shape, BF16), ml=DMA((6,)),
        stb=vmem((rows // 2, groups, 2 * STATE, chans // groups), BF16),
        held=vmem((nt, rows, width), BF16), f_s=DMA((nt,)), f_r=DMA((nt,)),
        gmv=vmem((nt, 1, width), F32),
        pout=vmem((nt, rows, width), BF16), arrived=vmem((nt, rows, width), BF16),
        m_s=DMA((nt,)), m_r=DMA((nt,)), mixed=vmem((rows, width), BF16),
        left=vmem((chans, depth), BF16), base=vmem((groups, depth, 2 * STATE), BF16),
    )
    scratch["sl"] = DMA((len(small),))
    for k, v in small.items():
        scratch["v." + k] = vmem(v.shape, v.dtype)
    for tag in ("1.", "2."):
        for k, v in half_scratch(nk, nt, rows, width, halfc).items():
            scratch[tag + k] = v
    names = list(small) + list(big) + ["out", "state_out"] + list(scratch)
    inside = pl.BlockSpec(memory_space=pltpu.VMEM)
    outside = pl.BlockSpec(memory_space=pl.ANY)
    out, state_out = pl.pallas_call(
        functools.partial(layer_kernel, nk, nt, names, list(small)),
        out_shape=(vmem(residual.shape, BF16), vmem(state.shape, F32)),
        in_specs=[outside] * (len(small) + len(big)),
        out_specs=(inside, inside),
        scratch_shapes=list(scratch.values()),
        compiler_params=pltpu.CompilerParams(
            collective_id=1, has_side_effects=True, vmem_limit_bytes=48 * 1024 * 1024),
        name="layer",
    )(*small.values(), *big.values())
    return pl.pallas_call(
        flush_kernel,
        out_shape=(jax.ShapeDtypeStruct(residual.shape, BF16),
                   jax.ShapeDtypeStruct(state.shape, F32)),
        in_specs=[inside] * 2,
        out_specs=(outside, outside),
        scratch_shapes=[DMA((9,))],
        compiler_params=pltpu.CompilerParams(vmem_limit_bytes=1024 * 1024),
        name="flush",
    )(out, state_out)


def solution(mesh):
    placed = (
        P("kv", "tp"),
        P("tp"),
        P("tp", "kv"),
        P("tp", "kv"),
        P("kv", "tp"),
        P(),
        P(None, "tp"),
        P(None, "tp"),
        P(None, "tp"),
        P(None, "tp"),
        P(None, "tp"),
        P("tp"),
        P("tp"),
        P("tp"),
        P(None, "tp"),
        P(None, "tp"),
        P(None, "tp"),
        P("kv", None, "tp"),
        P("kv", None, "tp"),
        P("kv", None, "tp"),
        P("kv", "tp", None, None),
        P("tp"),
        P("tp", None),
        P("tp"),
        P("tp", "kv"),
        P("tp", "kv"),
        P("kv", "tp"),
    )
    return jax.shard_map(
        functools.partial(per_device, mesh.shape["kv"], mesh.shape["tp"]),
        mesh=mesh,
        in_specs=placed,
        out_specs=(P("kv", "tp"), P("kv", "tp", None, None)),
        check_vma=False,
    )
```

```python
import functools

import jax
import jax.numpy as jnp
from jax import lax
from jax.experimental import pallas as pl
from jax.experimental.pallas import tpu as pltpu
from jax.sharding import PartitionSpec as P

HEAD_DIM = 64
STATE = 128
EPS = 1e-06
MESH = pl.DeviceIdType.MESH
F32 = jnp.float32
BF16 = jnp.bfloat16
DMA = pltpu.SemaphoreType.DMA


def silu(v):
    return v / (1.0 + jnp.exp(-v))


def dot(a, b):
    return jnp.dot(a, b, preferred_element_type=F32)


def dot_t(a, b, precision=None):
    return lax.dot_general(a, b, (((1,), (1,)), ((), ())), precision=precision,
                           preferred_element_type=F32)


def far_first(n):
    return sorted(range(1, n), key=lambda d: -min(d, n - d))


def remote(src, dst, send, recv, where):
    return pltpu.make_async_remote_copy(
        src_ref=src, dst_ref=dst, send_sem=send, recv_sem=recv,
        device_id=where, device_id_type=MESH,
    )


class Place:
    def __init__(self, nk, nt):
        self.nk, self.nt, self.nx = nk, nt, nt // 2
        self.kv, self.tp = lax.axis_index("kv"), lax.axis_index("tp")
        self.core = lax.rem(self.tp, 2)
        self.x = lax.div(self.tp, 2)
        self.partner = {"tp": self.tp + 1 - 2 * self.core}

    def kv_to(self, d):
        return lax.rem(self.kv + d, self.nk)

    def kv_from(self, d):
        return lax.rem(self.kv + self.nk - d, self.nk)

    def tp_to(self, d):
        return lax.rem(self.tp + d, self.nt)

    def tp_from(self, d):
        return lax.rem(self.tp + self.nt - d, self.nt)

    def x_to(self, e):
        return lax.rem(self.x + e, self.nx)

    def x_from(self, e):
        return lax.rem(self.x + self.nx - e, self.nx)

    def device(self, x, other):
        return 2 * x + (1 - self.core if other else self.core)

    def same_core(self, x):
        return {"tp": 2 * x + self.core}

    def cross_core(self, x):
        return {"tp": 2 * x + 1 - self.core}


def enter(p):
    barrier = pltpu.get_barrier_semaphore()
    for d in range(1, p.nk):
        pl.semaphore_signal(barrier, inc=1, device_id={"kv": p.kv_to(d)}, device_id_type=MESH)
    for d in range(1, p.nt):
        pl.semaphore_signal(barrier, inc=1, device_id={"tp": p.tp_to(d)}, device_id_type=MESH)
    pl.semaphore_wait(barrier, p.nk + p.nt - 2)


def half_scratch(nk, nt, rows, width, halfc):
    total, nx = nk * rows, nt // 2
    chunks, size = nk // nx, rows
    vmem = pltpu.VMEM
    return dict(
        wg=vmem((2, halfc, width), BF16), wu=vmem((2, halfc, width), BF16),
        wd=vmem((2, halfc, width), BF16), wl=DMA((4,)), ws=DMA((2,)), wr=DMA((2,)),
        xall=vmem((total, width), BF16), xg=vmem((2, total, width), BF16),
        sq=vmem((nx, chunks, 8, size), F32), sqr=vmem((nt, chunks, 8, size), F32),
        part=vmem((nx, chunks, 2, size, halfc), BF16),
        parr=vmem((nx, chunks, 2, size, halfc), BF16),
        mine=vmem((2, nk // nx * rows, halfc), F32),
        ahead=vmem((2, size, halfc), F32),
        hid=vmem((2, total, halfc), BF16),
        dpart=vmem((total, width), BF16), dparr=vmem((nk, rows, width), BF16),
        ag_s=DMA((nk,)), ag_r=DMA((nk,)), dd_s=DMA((nk,)), dd_r=DMA((nk,)),
        sq_s=DMA((nt, chunks)), sq_r=DMA((nt, chunks)),
        rs_s=DMA((nx, chunks)), rs_r=DMA((nx, chunks)),
        hx_s=DMA((nx, 2, chunks)), hx_r=DMA((nx, 2, chunks)),
        dn_s=DMA((nk,)), dn_r=DMA((nk,)),
    )


def local_weights(p, s, gate, lift, down):
    copies = [
        pltpu.make_async_copy(gate.at[p.core], s["wg"].at[0], s["wl"].at[0]),
        pltpu.make_async_copy(lift.at[p.core], s["wu"].at[0], s["wl"].at[1]),
        pltpu.make_async_copy(down.at[p.core], s["wd"].at[0], s["wl"].at[2]),
        pltpu.make_async_copy(down.at[1 - p.core], s["wd"].at[1], s["wl"].at[3]),
    ]
    for c in copies:
        c.start()
    return copies


def swap_weights(p, s, gate, lift):
    copies = [
        remote(gate.at[1 - p.core], s["wg"].at[1], s["ws"].at[0], s["wr"].at[0], p.partner),
        remote(lift.at[1 - p.core], s["wu"].at[1], s["ws"].at[1], s["wr"].at[1], p.partner),
    ]
    for c in copies:
        c.start()
    return copies


def flip_bits(v, m):
    out, bit = v, 1
    while bit <= m:
        if m & bit:
            out = out + bit * (1 - 2 * lax.rem(lax.div(v, bit), 2))
        bit *= 2
    return out


def half_step(p, s, x_ref, gain, local, swapped, idle, tag=''):
    nk, nt, nx = p.nk, p.nt, p.nx
    rows, width = x_ref.shape
    per = nk // nx
    chunks, size = per, rows
    features = width * nt
    near = lax.div(p.kv, nx)
    order = [flip_bits(near, i) for i in range(chunks)]
    peers = far_first(nx)
    sends = []

    def block(k):
        spot = lax.rem(k, nx) * per + lax.div(k, nx)
        return pl.ds(pl.multiple_of(spot * rows, rows), rows)

    def chunk(x, i):
        return pl.ds(pl.multiple_of((x * per + order[i]) * rows, size), size)

    def member(x, i):
        return order[i] * nx + x
    for m in range(1, nk):
        c = remote(x_ref, s["xall"].at[block(p.kv)], s["ag_s"].at[m], s["ag_r"].at[p.kv],
                   {"kv": flip_bits(p.kv, m)})
        c.start()
        sends.append(c)
    s["xall"][block(p.kv), :] = x_ref[...]
    idle[0]()

    def landed(ref, sem):
        pltpu.make_async_copy(ref, ref, sem).wait()

    def arrive(k):
        at = block(k)

        @pl.when(k != p.kv)
        def _():
            landed(s["xall"].at[at], s["ag_r"].at[k])

        value = s["xall"][at, :].astype(F32)
        s["xg"][0, at, :] = (value * gain).astype(BF16)
        remote(s["xg"].at[0, at], s["xg"].at[1, at], s["dd_s"].at[k], s["dd_r"].at[k],
               p.partner).start()
        value = value * value
        folded = value[:, :128]
        for i in range(128, width, 128):
            folded = folded + value[:, i:i + 128]
        return jnp.broadcast_to(jnp.sum(jnp.transpose(folded), axis=0, keepdims=True), (8, rows))

    def ready(k):
        landed(s["xg"].at[1, block(k)], s["dd_r"].at[k])

    squares, parts = {}, {}

    def collect(i):
        for e in peers + [0]:
            to = p.x_to(e)
            s["sq"][e, i] = arrive(member(to, i))
            for other in range(2):
                if e or other:
                    where = p.same_core(to) if not other else p.cross_core(to)
                    c = remote(s["sq"].at[e, i], s["sqr"].at[2 * e + other, i],
                               s["sq_s"].at[2 * e + other, i], s["sq_r"].at[2 * e + other, i],
                               where)
                    c.start()
                    squares[2 * e + other, i] = c
    collect(0)
    for i in range(chunks):
        if i + 1 < chunks:
            collect(i + 1)
        if i == 0:
            local[0].wait()
            local[1].wait()
            for c in swapped:
                c.wait_recv()
        for e in peers:
            to = p.x_to(e)
            at = chunk(to, i)
            for j, w in enumerate((s["wg"], s["wu"])):
                s["ahead"][j] = dot_t(s["xg"][0, at, :], w[0])
            ready(member(to, i))
            for j, w in enumerate((s["wg"], s["wu"])):
                s["part"][e, i, j] = (s["ahead"][j]
                                      + dot_t(s["xg"][1, at, :], w[1])).astype(BF16)
            c = remote(s["part"].at[e, i], s["parr"].at[e, i], s["rs_s"].at[e, i],
                       s["rs_r"].at[e, i], p.same_core(to))
            c.start()
            parts[e, i] = c
    for i in range(chunks):
        ready(member(p.x, i))
    whole = pl.ds(pl.multiple_of(p.x * per * rows, rows), per * rows)
    for j, w in enumerate((s["wg"], s["wu"])):
        s["mine"][j] = dot_t(s["xg"][0, whole, :], w[0]) + dot_t(s["xg"][1, whole, :], w[1])
    sends += list(squares.values()) + list(parts.values())
    idle[1]()
    spread = {}
    for i in range(chunks):
        sq = s["sq"][0, i]
        for n in range(1, nt):
            squares[n, i].wait_recv()
            sq = sq + s["sqr"][n, i]
        factor = jnp.transpose(lax.rsqrt(sq / features + EPS))[:, :1]
        own = pl.ds(pl.multiple_of(order[i] * rows, rows), rows)
        gate, lift = s["mine"][0, own, :], s["mine"][1, own, :]
        for e in reversed(peers):
            parts[e, i].wait_recv()
            gate = gate + s["parr"][e, i, 0].astype(F32)
            lift = lift + s["parr"][e, i, 1].astype(F32)
        at = chunk(p.x, i)
        s["hid"][0, at, :] = (silu(gate * factor) * (lift * factor)).astype(BF16)
        for e in peers + [0]:
            for other in range(2):
                if e or other:
                    to = p.x_to(e)
                    where = p.same_core(to) if not other else p.cross_core(to)
                    c = remote(s["hid"].at[0, at], s["hid"].at[other, at],
                               s["hx_s"].at[e, other, i], s["hx_r"].at[e, other, i], where)
                    c.start()
                    spread[e, other, i] = c
    sends += spread.values()
    local[2].wait()
    local[3].wait()
    for e in [0] + list(reversed(peers)):
        source = p.x_from(e)
        if e == (peers or [0])[-1]:
            idle[2]()
        for i in range(chunks):
            at = chunk(source, i)
            if e:
                spread[e, 0, i].wait_recv()
            spread[e, 1, i].wait_recv()
            mid = dot(s["hid"][0, at, :], s["wd"][0]) + dot(s["hid"][1, at, :], s["wd"][1])
            s["dpart"][at, :] = mid.astype(BF16)
            to = member(source, i)

            @pl.when(to != p.kv)
            def _():
                remote(s["dpart"].at[block(to)], s["dparr"].at[p.kv], s["dn_s"].at[to],
                       s["dn_r"].at[p.kv], {"kv": to}).start()
    idle[3]()
    acc = s["dpart"][block(p.kv), :].astype(F32)
    for m in range(1, nk):
        source = flip_bits(p.kv, m)
        landed(s["dparr"].at[source], s["dn_r"].at[source])
        acc = acc + s["dparr"][source].astype(F32)
    def finish():
        for m in range(1, nk):
            to = flip_bits(p.kv, m)
            landed(s["dparr"].at[to], s["dn_s"].at[to])
        for k in range(nk):
            landed(s["xg"].at[1, block(k)], s["dd_s"].at[k])
        for c in sends + swapped:
            c.wait_send()

    return x_ref[...].astype(F32) + 0.5 * acc, finish


def conv(taps_ref, buf_ref, newest):
    taps = taps_ref[...].astype(F32)
    count = taps.shape[0]
    old = buf_ref[...].astype(F32)
    acc = newest.astype(BF16).astype(F32) * taps[count - 1:count]
    for k in range(count - 1):
        acc = acc + old[k] * taps[k:k + 1]
    return silu(acc)


def split(v):
    high = v.astype(BF16).astype(F32)
    return high, v - high


def layer_kernel(nk, nt, names, small, *refs):
    tag = 'k_'
    r = dict(zip(names, refs))
    p = Place(nk, nt)
    one = {k[2:]: v for k, v in r.items() if k.startswith("1.")}
    two = {k[2:]: v for k, v in r.items() if k.startswith("2.")}
    state = r["state_out"]
    smalls = {}
    for i, name in enumerate(small):
        smalls[name] = pltpu.make_async_copy(r[name], r["v." + name], r["sl"].at[i])
        smalls[name].start()
        r[name] = r["v." + name]
    x_ref = r["x"]
    rows, width = x_ref.shape
    features = nt * width
    chans = r["wx"].shape[-1]
    gs = r["wb"].shape[-1]
    heads = r["ws"].shape[0]
    groups = gs // STATE
    gch = chans // groups
    hg = heads // groups
    wcat = r["wcat"]
    local1 = local_weights(p, one, r["gate1"], r["lift1"], r["down1"])
    mixload = []
    at = 0
    for i, name in enumerate(("wz", "wx", "wb", "wr")):
        w = r[name]
        c = pltpu.make_async_copy(w, wcat.at[:, :, at:at + w.shape[-1]], r["ml"].at[i])
        at += w.shape[-1]
        mixload.append(c)
    mixload.append(pltpu.make_async_copy(r["wo"], r["wov"], r["ml"].at[4]))
    stateload = pltpu.make_async_copy(r["state"], state, r["ml"].at[5])
    stateload.start()
    enter(p)
    smalls["x"].wait()
    smalls["g1"].wait()
    swap1 = swap_weights(p, one, r["gate1"], r["lift1"])

    def row(name):
        return r[name][...].astype(F32).reshape(1, -1)

    later = {}

    def load_rest():
        for c in mixload:
            c.start()
        later["local"] = local_weights(p, two, r["gate2"], r["lift2"], r["down2"])
        narrow()

    def narrow():
        stateload.wait()

        def body(i, _):
            for g in range(groups):
                for j in range(2):
                    old = state[2 * i + j, g * hg:(g + 1) * hg].reshape(gch, STATE)
                    r["stb"][i, g, j * STATE:(j + 1) * STATE, :] = jnp.transpose(old).astype(BF16)
            return 0

        lax.fori_loop(0, rows // 2, body, 0)

    def swap_rest():
        later["swap"] = swap_weights(p, two, r["gate2"], r["lift2"])

    def nothing():
        pass

    first, finish1 = half_step(p, one, x_ref, row("g1"), local1, swap1,
                               (load_rest, swap_rest, nothing, nothing), 'a_')
    held = r["held"]
    held[p.tp] = first.astype(BF16)
    copies = {}
    others = [(e, o) for e in far_first(p.nx) for o in range(2)] + [(0, 1)]
    for e, o in others:
        n = 2 * e + o
        c = remote(held.at[p.tp], held.at[p.tp], r["f_s"].at[n], r["f_r"].at[n],
                   {"tp": p.device(p.x_to(e), o)})
        c.start()
        copies[n] = c
    for c in mixload:
        c.wait()
    for name in small[2:]:
        smalls[name].wait()
    gm = row("gm")
    gmv = r["gmv"]
    for t in range(nt):
        gmv[t] = gm[:, t * width:(t + 1) * width]
    total = jnp.zeros((rows, 1), F32)
    proj = jnp.zeros((rows, wcat.shape[-1]), F32)
    raw = jnp.zeros((rows, heads), F32)
    for e, o in [(0, 0), (0, 1)] + others[:-1]:
        t = p.device(p.x_from(e), o)
        if e or o:
            copies[2 * e + o].wait_recv()
        v = held[t].astype(F32)
        total = total + jnp.sum(v * v, axis=1, keepdims=True)
        scaled = (v * gmv[t]).astype(BF16)
        proj = proj + dot(scaled, wcat[t])
        raw = raw + dot_t(scaled, r["ws"][:, pl.ds(pl.multiple_of(t * width, width), width)])
    factor = lax.rsqrt(total / features + EPS)
    proj = proj * factor
    raw = (raw * factor).astype(BF16).astype(F32) + r["bias"][...]

    def spread(v):
        a = lax.broadcasted_iota(jnp.int32, (heads, chans), 0)
        c = lax.broadcasted_iota(jnp.int32, (heads, chans), 1)
        ind = jnp.where(c // HEAD_DIM == a, 1.0, 0.0).astype(F32)
        return jnp.dot(v, ind, precision=lax.Precision.HIGHEST, preferred_element_type=F32)

    z = proj[:, :chans].astype(BF16).astype(F32)
    xc = conv(r["tx"], r["bx"], proj[:, chans:2 * chans])
    bc = conv(r["tb"], r["bb"], proj[:, 2 * chans:2 * chans + gs])
    rc = conv(r["tr"], r["br"], proj[:, 2 * chans + gs:])
    step = jnp.maximum(raw, 0.0) + jnp.log1p(jnp.exp(-jnp.abs(raw)))
    retain = jnp.exp(-step * jnp.exp(r["rate"][...]))
    sx = spread(step) * xc
    keep = spread(retain)
    rowid = lax.broadcasted_iota(jnp.int32, (rows, 2 * STATE), 0)
    colid = lax.broadcasted_iota(jnp.int32, (rows, 2 * STATE), 1) // STATE
    pieces = []
    for g in range(groups):
        rg = rc[:, g * STATE:(g + 1) * STATE]
        twice = jnp.concatenate([rg, rg], axis=1)
        acc = jnp.zeros((rows, gch), F32)
        for i in range(rows // 2):
            lhs = jnp.where(rowid - colid == 2 * i, twice, 0.0).astype(BF16)
            acc = acc + dot(lhs, r["stb"][i, g])
        br = jnp.sum(bc[:, g * STATE:(g + 1) * STATE] * rg, axis=1, keepdims=True)
        pieces.append(acc * keep[:, g * gch:(g + 1) * gch] + sx[:, g * gch:(g + 1) * gch] * br)
    out = jnp.concatenate(pieces, axis=1) + spread(r["skip"][...]) * xc
    gated = out.astype(BF16).astype(F32) * silu(z)
    pieces = []
    for g in range(groups):
        v = gated[:, g * gch:(g + 1) * gch]
        pieces.append(v * lax.rsqrt(jnp.mean(v * v, axis=1, keepdims=True) + EPS))
    gated = (jnp.concatenate(pieces, axis=1) * row("gg")).astype(BF16)
    pout, arrived = r["pout"], r["arrived"]
    outs = {}
    for e, o in others + [(0, 0)]:
        d = 2 * e + o
        to = p.device(p.x_to(e), o)
        wo = r["wov"][:, pl.ds(pl.multiple_of(to * width, width), width)]
        pout[d] = dot(gated, wo).astype(BF16)
        if d:
            c = remote(pout.at[d], arrived.at[d], r["m_s"].at[d], r["m_r"].at[d], {"tp": to})
            c.start()
            outs[d] = c
    depth = r["base"].shape[1]
    pad = depth - 3 * rows
    re_hi, re_lo = split(keep)
    left = jnp.concatenate([sx, re_hi, re_lo, jnp.zeros((pad, chans), F32)], axis=0)
    r["left"][...] = left.T.astype(BF16)
    for g in range(groups):
        zero = jnp.zeros((2 * rows + pad, STATE), F32)
        full = jnp.ones((2 * rows, STATE), F32)
        r["base"][g, :, :STATE] = jnp.concatenate(
            [bc[:, g * STATE:(g + 1) * STATE], zero], axis=0).astype(BF16)
        r["base"][g, :, STATE:] = jnp.concatenate(
            [zero[:rows], full, zero[:pad]], axis=0).astype(BF16)
    acc = held[p.tp].astype(F32) + pout[0].astype(F32)
    for d in outs:
        outs[d].wait_recv()
        acc = acc + arrived[d].astype(F32)
    r["mixed"][...] = acc.astype(BF16)

    rowmod = lax.rem(lax.broadcasted_iota(jnp.int32, (depth, 2 * STATE), 0), rows)

    def update(low, high):
        many = 4 if (high - low) % 4 == 0 else 1

        def body(n, _):
            for j in range(many):
                b = low + n * many + j
                mask = jnp.where(rowmod == b, 1.0, 0.0).astype(BF16)
                for g in range(groups):
                    right = r["base"][g] * mask
                    both = dot(r["left"][g * gch:(g + 1) * gch, :], right)
                    old = state[b, g * hg:(g + 1) * hg].reshape(gch, STATE)
                    new = both[:, STATE:] * old + both[:, :STATE]
                    state[b, g * hg:(g + 1) * hg] = new.reshape(hg, HEAD_DIM, STATE)
            return 0

        return lambda: lax.fori_loop(0, (high - low) // many, body, 0)

    cuts = [rows * n // 16 for n in (0, 10, 12, 16, 16)]
    last, finish2 = half_step(p, two, r["mixed"], row("g2"), later["local"], later["swap"],
                              tuple(update(cuts[n], cuts[n + 1]) for n in range(4)), 'b_')
    r["out"][...] = last.astype(BF16)
    finish1()
    finish2()
    for c in list(copies.values()) + list(outs.values()):
        c.wait_send()


def flush_kernel(a, b, oa, ob, sem):
    pieces = sem.shape[0] - 1
    step = b.shape[0] // pieces
    copies = [pltpu.make_async_copy(a, oa, sem.at[pieces])]
    for i in range(pieces):
        at = pl.ds(i * step, step)
        copies.append(pltpu.make_async_copy(b.at[at], ob.at[at], sem.at[i]))
    for c in copies:
        c.start()
    for c in copies:
        c.wait()


def per_device(nk, nt, residual, first_gain, first_gate, first_lift, first_down,
               mixer_gain, wz, wx, wb, wr, ws, bias, rate, skip, tx, tb, tr, bx, bb, br,
               state, group_gain, wo, second_gain, second_gate, second_lift, second_down):
    rows, width = residual.shape
    halfc = first_gate.shape[1] // 2
    chans, heads = wx.shape[1], ws.shape[1]
    groups = wb.shape[1] // STATE
    vmem = pltpu.VMEM

    def tall(w):
        return w.T.reshape(2, halfc, width)

    def flip(v):
        return jnp.transpose(v, (1, 0, 2))

    small = dict(x=residual, g1=first_gain, g2=second_gain, gm=mixer_gain, gg=group_gain,
                 ws=ws.T, bias=bias[None, :], rate=rate[None, :], skip=skip[None, :],
                 tx=tx, tb=tb, tr=tr, bx=flip(bx), bb=flip(bb), br=flip(br))
    big = dict(gate1=tall(first_gate), lift1=tall(first_lift),
               down1=first_down.reshape(2, halfc, width),
               gate2=tall(second_gate), lift2=tall(second_lift),
               down2=second_down.reshape(2, halfc, width),
               wz=wz.reshape(nt, width, -1), wx=wx.reshape(nt, width, -1),
               wb=wb.reshape(nt, width, -1), wr=wr.reshape(nt, width, -1), wo=wo, state=state)
    depth = -(-3 * rows // 128) * 128
    scratch = dict(
        wcat=vmem((nt, width, 2 * chans + 2 * groups * STATE), BF16),
        wov=vmem(wo.shape, BF16), ml=DMA((6,)),
        stb=vmem((rows // 2, groups, 2 * STATE, chans // groups), BF16),
        held=vmem((nt, rows, width), BF16), f_s=DMA((nt,)), f_r=DMA((nt,)),
        gmv=vmem((nt, 1, width), F32),
        pout=vmem((nt, rows, width), BF16), arrived=vmem((nt, rows, width), BF16),
        m_s=DMA((nt,)), m_r=DMA((nt,)), mixed=vmem((rows, width), BF16),
        left=vmem((chans, depth), BF16), base=vmem((groups, depth, 2 * STATE), BF16),
    )
    scratch["sl"] = DMA((len(small),))
    for k, v in small.items():
        scratch["v." + k] = vmem(v.shape, v.dtype)
    for tag in ("1.", "2."):
        for k, v in half_scratch(nk, nt, rows, width, halfc).items():
            scratch[tag + k] = v
    names = list(small) + list(big) + ["out", "state_out"] + list(scratch)
    inside = pl.BlockSpec(memory_space=pltpu.VMEM)
    outside = pl.BlockSpec(memory_space=pl.ANY)
    out, state_out = pl.pallas_call(
        functools.partial(layer_kernel, nk, nt, names, list(small)),
        out_shape=(vmem(residual.shape, BF16), vmem(state.shape, F32)),
        in_specs=[outside] * (len(small) + len(big)),
        out_specs=(inside, inside),
        scratch_shapes=list(scratch.values()),
        compiler_params=pltpu.CompilerParams(
            collective_id=1, has_side_effects=True, vmem_limit_bytes=48 * 1024 * 1024),
        name="layer",
    )(*small.values(), *big.values())
    return pl.pallas_call(
        flush_kernel,
        out_shape=(jax.ShapeDtypeStruct(residual.shape, BF16),
                   jax.ShapeDtypeStruct(state.shape, F32)),
        in_specs=[inside] * 2,
        out_specs=(outside, outside),
        scratch_shapes=[DMA((9,))],
        compiler_params=pltpu.CompilerParams(vmem_limit_bytes=1024 * 1024),
        name="flush",
    )(out, state_out)


def solution(mesh):
    placed = (
        P("kv", "tp"),
        P("tp"),
        P("tp", "kv"),
        P("tp", "kv"),
        P("kv", "tp"),
        P(),
        P(None, "tp"),
        P(None, "tp"),
        P(None, "tp"),
        P(None, "tp"),
        P(None, "tp"),
        P("tp"),
        P("tp"),
        P("tp"),
        P(None, "tp"),
        P(None, "tp"),
        P(None, "tp"),
        P("kv", None, "tp"),
        P("kv", None, "tp"),
        P("kv", None, "tp"),
        P("kv", "tp", None, None),
        P("tp"),
        P("tp", None),
        P("tp"),
        P("tp", "kv"),
        P("tp", "kv"),
        P("kv", "tp"),
    )
    return jax.shard_map(
        functools.partial(per_device, mesh.shape["kv"], mesh.shape["tp"]),
        mesh=mesh,
        in_specs=placed,
        out_specs=(P("kv", "tp"), P("kv", "tp", None, None)),
        check_vma=False,
    )
```
